512 devices in a mesh: ep: 32 (over z, core), tp: 16 (over y, x).
Axes of the slice: x: 4, y: 4, z: 16, core: 2. Of those that a mesh axis runs over, the one named last changes fastest.
Arguments:
- mix_in: bfloat16 [8192, 2048], P('ep'), may hold values from -6 to 6
- mix_gain: float32 [2048], replicated, may hold values from 0.1 to 1.9
- w_in_x: bfloat16 [2048, 2048], P(None, 'tp'), may hold values from -0.125 to 0.125
- w_in_y: bfloat16 [2048, 2048], P(None, 'tp'), may hold values from -0.125 to 0.125
- conv_taps: float32 [4, 2048], P(None, 'tp'), may hold values from -3 to 3
- recur_gate_w: bfloat16 [16, 128, 128], P('tp'), may hold values from -0.5 to 0.5
- input_gate_w: bfloat16 [16, 128, 128], P('tp'), may hold values from -0.5 to 0.5
- decay_logit: float32 [2048], P('tp'), may hold values from 4 to 20
- decay_shift: float32 [8192, 2048], P('ep', 'tp'), may hold values from -2.2 to 0
- moe_in: bfloat16 [8192, 2048], P('ep'), may hold values from -6 to 6
- moe_gain: float32 [2048], replicated, may hold values from 0.1 to 1.9
- routes: int32 [8192, 2], P('ep'), may hold values from 0 to 31, all different within a row; in each aligned block of 256 rows (0 to 255, 256 to 511, ...) at most 32 rows name the same one
- route_weight: float32 [8192, 2], P('ep'), may hold values from 0.1 to 1
- expert_gate: bfloat16 [32, 2048, 2048], P('ep', None, 'tp'), may hold values from -0.125 to 0.125
- expert_up: bfloat16 [32, 2048, 2048], P('ep', None, 'tp'), may hold values from -0.125 to 0.125
- expert_down: bfloat16 [32, 2048, 2048], P('ep', None, 'tp'), may hold values from -0.125 to 0.125
Outputs:
- mixer_out: bfloat16 [8192, 2048], P('ep', 'tp')
- moe_out: bfloat16 [8192, 2048], P('ep', 'tp')
The draws below stay inside these ranges and needn't reach their ends.
Inputs may be any that keep to these rules, and one draw needn't show every extreme that they name: `routes`: each row names 2 different experts. Among the rows of one index of ep no expert is named more than 32 times, a bound that some block reaches.
All inputs are finite; a program needn't handle non-finite values.
Results may differ from the reference program's by a relative error of at most 0.0095.
Values may be sent and summed in bfloat16 or wider, within the bound.
A program may use at most 64 MiB of HBM per device.

```python
import math
import jax
import jax.numpy as jnp
import numpy as np
from jax import lax

D = 2048
FILTER_SECTIONS = 16
SECTION_FEATURES = 128
KCONV = 4
FF = 2048
TOPK = 2
TOK_DEV = 256
SUBBATCH_SPAN = 8192
WIDTH = 2048
EXPERTS = 32
CAP = 32
N_EP = 32


def draw_decay_logit(key, part):
    pick_key, slow_key, fast_key, jitter_key = jax.random.split(jax.random.fold_in(key, 11), 4)
    fast_head = jax.random.uniform(pick_key, (FILTER_SECTIONS,)) < 0.5
    slow_rate = jnp.exp(jax.random.uniform(slow_key, (FILTER_SECTIONS,), minval=math.log(0.2), maxval=math.log(0.6))) / SUBBATCH_SPAN
    fast_rate = jnp.exp(jax.random.uniform(fast_key, (FILTER_SECTIONS,), minval=math.log(0.01), maxval=math.log(1.0 / 30.0)))
    head_rate = jnp.where(fast_head, fast_rate, slow_rate)
    jitter = jax.random.uniform(jitter_key, (FILTER_SECTIONS, SECTION_FEATURES), minval=0.7, maxval=1.4)
    softened = (head_rate[:, None] * jitter / 4.0).reshape(FILTER_SECTIONS * SECTION_FEATURES)
    return -jnp.log(jnp.expm1(softened))


def draw_decay_shift(key, part):
    block_key, chan_key, place_key, depth_key = jax.random.split(jax.random.fold_in(key, 23), 4)
    blocks = SUBBATCH_SPAN // TOK_DEV
    spread = math.log(2.0)
    factor = jnp.exp(jax.random.uniform(block_key, (blocks,), minval=-spread, maxval=spread))
    channel = jax.random.uniform(chan_key, (FILTER_SECTIONS * SECTION_FEATURES,), minval=0.2, maxval=0.8)
    stationary_regime = -jnp.repeat(factor, TOK_DEV)[:, None] * channel[None, :] / SUBBATCH_SPAN
    assignment_seats = jax.random.randint(place_key, (3, FILTER_SECTIONS), 0, SUBBATCH_SPAN)
    stack_levels = jnp.log1p(-jax.random.uniform(depth_key, (3, FILTER_SECTIONS), minval=0.2, maxval=0.5))
    sequence_offsets = jnp.arange(SUBBATCH_SPAN)[:, None]
    packet_clusters = jnp.zeros((SUBBATCH_SPAN, FILTER_SECTIONS), jnp.float32)
    for picked_ordinal in range(3):
        packet_clusters = packet_clusters + jnp.where(sequence_offsets == assignment_seats[picked_ordinal][None, :], stack_levels[picked_ordinal][None, :], 0.0)
    return stationary_regime + jnp.repeat(packet_clusters, SECTION_FEATURES, axis=1)


def shard_levels(rng, shape, shards, least, high):
    factor_of = 1.0
    for axis_at, parts in shards:
        heights = jax.random.uniform(jax.random.fold_in(jax.random.fold_in(rng, 6), axis_at), (parts,), jnp.float32, least / len(shards), high / len(shards))
        factor_of = factor_of * jnp.repeat(jnp.exp(heights), shape[axis_at] // parts).reshape((-1,) + (1,) * (len(shape) - 1 - axis_at))
    return factor_of


def assign_block(rng, own, number, rows, amount, top, most, skew):
    sequence = jax.random.permutation(rng, amount)
    crowded, common = load_shares(amount, rows * top, most, skew, True), load_shares(amount, rows * top, most, skew, False)
    places = jnp.arange(amount)

    def named(sizes, offset_by):
        used = int((sizes > 0).sum())
        fixed = max(1, used // 4)
        passed = fixed + (places - fixed + offset_by * (used - fixed)) % max(1, amount - fixed)
        return jnp.zeros((amount,), jnp.int32).at[sequence[jnp.where(places < fixed, places, passed)]].set(jnp.asarray(sizes, jnp.int32))

    sizes = jnp.where(number % 4 == 0, named(crowded, number // 4), named(common, number - number // 4 - 1))
    mixed = jax.random.permutation(jax.random.fold_in(own, 3), amount)
    giver, taker = mixed[0:amount // 2 * 2:2], mixed[1:amount // 2 * 2:2]
    slack = jnp.minimum(sizes[giver] - 1, most - sizes[taker]) // 2
    slack = jnp.where((giver == sequence[0]) | (taker == sequence[0]) | (sizes[taker] == 0), 0, jnp.maximum(slack, 0))
    passed = jax.random.randint(jax.random.fold_in(own, 4), (amount // 2,), 0, 1 << 20) % (slack + 1)
    sizes = sizes.at[giver].add(-passed).at[taker].add(passed)
    labels = jnp.searchsorted(jnp.cumsum(sizes), jnp.arange(rows * top), side="right").astype(jnp.int32)
    listing = labels.reshape(top, rows).T
    listing = listing[jax.random.permutation(jax.random.fold_in(own, 1), rows)]
    offset_by = jax.random.randint(jax.random.fold_in(own, 2), (rows, 1), 0, top)
    return jnp.take_along_axis(listing, (jnp.arange(top)[None, :] + offset_by) % top, axis=1)


def load_shares(number_of, total, most, slope, full):
    portions = [(1 << 20) // math.isqrt(grade ** slope) + 1 for grade in range(1, number_of + 1)]
    largest = most if full else min(most, max(-(-total // number_of), total * portions[0] // sum(portions)))
    least = 1 if total - largest >= number_of - 1 else 0
    holding, spare = [largest] + [least] * (number_of - 1), total - largest - least * (number_of - 1)
    while spare > 0:
        free = [i for i in range(1, number_of) if holding[i] < largest] or [i for i in range(1, number_of) if holding[i] < most]
        mass, remaining = sum([portions[i] for i in free]), spare
        for i in free:
            more = min(most - holding[i], max(1, remaining * portions[i] // mass), spare)
            holding[i] = holding[i] + more
            spare = spare - more
    return np.array(holding)


def noise(rng, shape, scale, bound, shards=(), held_as=jnp.bfloat16):
    level = shard_levels(rng, shape, shards, -0.22, 0.18) if shards else 1.0
    drawn = jax.random.normal(rng, shape, jnp.float32) * scale * level
    return jnp.minimum(jnp.maximum(drawn, -bound), bound).astype(held_as)


def setup_inputs(seed: int = 0) -> dict:
    keys = jax.random.split(jax.random.key(seed), 17)
    mix_in = noise(keys[0], (SUBBATCH_SPAN, D), 1.0, 6.0, ((0, 32),))
    mix_gain = jnp.clip(1.0 + 0.18 * jax.random.normal(keys[1], (D,), jnp.float32), 0.1, 1.9)
    w_in_x = noise(keys[2], (D, WIDTH), D ** -0.5, 0.125, ((1, 16),))
    w_in_y = noise(keys[3], (D, WIDTH), D ** -0.5, 0.125, ((1, 16),))
    conv_taps = noise(keys[4], (KCONV, WIDTH), 0.5, 3.0, ((1, 16),), jnp.float32)
    recur_gate_w = noise(keys[5], (FILTER_SECTIONS, SECTION_FEATURES, SECTION_FEATURES), SECTION_FEATURES ** -0.5, 0.5, ((0, 16),))
    input_gate_w = noise(keys[6], (FILTER_SECTIONS, SECTION_FEATURES, SECTION_FEATURES), SECTION_FEATURES ** -0.5, 0.5, ((0, 16),))
    decay_logit = draw_decay_logit(jax.random.fold_in(keys[16], 71), 0)
    decay_shift = draw_decay_shift(jax.random.fold_in(keys[16], 71), 0)
    moe_in = noise(keys[9], (SUBBATCH_SPAN, D), 1.0, 6.0, ((0, 32),))
    moe_gain = jnp.clip(1.0 + 0.18 * jax.random.normal(keys[10], (D,), jnp.float32), 0.1, 1.9)
    routes_keys = jax.random.split(jax.random.fold_in(keys[11], 1), SUBBATCH_SPAN // TOK_DEV)
    routes_turns = jax.random.permutation(jax.random.fold_in(keys[11], 3), SUBBATCH_SPAN // TOK_DEV)
    routes = jax.vmap(lambda own, number: assign_block(jax.random.fold_in(keys[11], 2), own, number, TOK_DEV, EXPERTS, TOPK, CAP, 2))(routes_keys, routes_turns).reshape((SUBBATCH_SPAN, TOPK))
    route_weight = jnp.clip(jnp.exp(math.log(1.0) - 2.3025851 * jax.random.uniform(keys[12], (SUBBATCH_SPAN, TOPK), jnp.float32) ** shard_levels(keys[12], (SUBBATCH_SPAN, TOPK), ((0, 32),), -0.2, 0.2)), 0.1, 1.0)
    expert_gate = noise(keys[13], (EXPERTS, D, FF), D ** -0.5, 0.125, ((0, 32), (2, 16)))
    expert_up = noise(keys[14], (EXPERTS, D, FF), D ** -0.5, 0.125, ((0, 32), (2, 16)))
    expert_down = noise(keys[15], (EXPERTS, FF, D), FF ** -0.5, 0.125, ((0, 32), (2, 16)))
    return {"mix_in": mix_in, "mix_gain": mix_gain, "w_in_x": w_in_x, "w_in_y": w_in_y, "conv_taps": conv_taps, "recur_gate_w": recur_gate_w, "input_gate_w": input_gate_w, "decay_logit": decay_logit, "decay_shift": decay_shift, "moe_in": moe_in, "moe_gain": moe_gain, "routes": routes, "route_weight": route_weight, "expert_gate": expert_gate, "expert_up": expert_up, "expert_down": expert_down}


epsilon = 1e-06
lru_scale = 8.0

def norm_rows(rows, gain):
    widened = rows.astype(jnp.float32)
    scaled = widened * lax.rsqrt(lax.optimization_barrier(jnp.mean(widened * widened, axis=-1, keepdims=True)) + epsilon)
    return (scaled * gain.astype(jnp.float32)[None, :]).astype(jnp.bfloat16)

def link(earlier, later):
    return (earlier[0] * later[0], later[0] * earlier[1] + later[1])

def reference(mix_in, mix_gain, w_in_x, w_in_y, conv_taps, recur_gate_w, input_gate_w, decay_logit, decay_shift, moe_in, moe_gain, routes, route_weight, expert_gate, expert_up, expert_down):
    mixer_rows = norm_rows(mix_in, mix_gain)
    x_branch = jnp.dot(mixer_rows, w_in_x, preferred_element_type=jnp.float32).astype(jnp.bfloat16)
    y_branch = jnp.dot(mixer_rows, w_in_y, preferred_element_type=jnp.float32).astype(jnp.bfloat16)
    padded = jnp.concatenate([jnp.zeros((KCONV - 1, WIDTH), jnp.bfloat16), x_branch], axis=0)
    conv_sum = jnp.zeros((SUBBATCH_SPAN, WIDTH), jnp.float32)
    for tap_index in range(KCONV):
        conv_sum = conv_sum + conv_taps[tap_index][None, :].astype(jnp.float32) * padded[tap_index:tap_index + SUBBATCH_SPAN].astype(jnp.float32)
    x_conv = conv_sum.astype(jnp.bfloat16)
    heads_in = x_conv.astype(jnp.float32).reshape(SUBBATCH_SPAN, FILTER_SECTIONS, SECTION_FEATURES)
    gate_a = jnp.einsum('thi,hij->thj', heads_in, recur_gate_w.astype(jnp.float32)).reshape(SUBBATCH_SPAN, WIDTH)
    gate_x = jnp.einsum('thi,hij->thj', heads_in, input_gate_w.astype(jnp.float32)).reshape(SUBBATCH_SPAN, WIDTH)
    log_decay = -lru_scale * jax.nn.sigmoid(gate_a) * jax.nn.softplus(-decay_logit)[None, :] + decay_shift
    lru_drive = jnp.sqrt(-jnp.expm1(2.0 * log_decay)) * jax.nn.sigmoid(gate_x) * x_conv.astype(jnp.float32)
    through, lru_state = lax.associative_scan(link, (jnp.exp(log_decay), lru_drive), axis=0)
    mixer_out = (lru_state * jax.nn.gelu(y_branch.astype(jnp.float32))).astype(jnp.bfloat16)
    moe_rows = norm_rows(moe_in, moe_gain)
    grouped = routes.reshape(N_EP, TOK_DEV * TOPK)
    onehot = (grouped[:, :, None] == jnp.arange(EXPERTS, dtype=jnp.int32)[None, None, :]).astype(jnp.int32)
    slot_rank = lax.optimization_barrier(jnp.sum(jnp.cumsum(onehot, axis=1) * onehot, axis=2)) - 1
    source = jnp.broadcast_to(jnp.arange(N_EP, dtype=jnp.int32)[:, None], slot_rank.shape)
    slot_index = (source * CAP + slot_rank).reshape(-1).astype(jnp.int32)
    expert_ids = routes.reshape(-1).astype(jnp.int32)
    token_index = jnp.repeat(jnp.arange(SUBBATCH_SPAN, dtype=jnp.int32), TOPK)
    table = jnp.zeros((EXPERTS, N_EP * CAP, D), jnp.bfloat16).at[expert_ids, slot_index].set(moe_rows[token_index])

    def run_expert(packed):
        rows_in, gate_w, up_w, down_w = packed
        gate_proj = jnp.dot(rows_in, gate_w, preferred_element_type=jnp.float32)
        up_proj = jnp.dot(rows_in, up_w, preferred_element_type=jnp.float32)
        hidden = (jax.nn.silu(gate_proj) * up_proj).astype(jnp.bfloat16)
        return jnp.dot(hidden, down_w, preferred_element_type=jnp.float32).astype(jnp.bfloat16)
    results = lax.map(run_expert, (table, expert_gate, expert_up, expert_down))
    picked = results[expert_ids, slot_index].astype(jnp.float32).reshape(SUBBATCH_SPAN, TOPK, D)
    route_share = route_weight / lax.optimization_barrier(jnp.sum(route_weight, axis=1, keepdims=True))
    moe_out = lax.optimization_barrier(jnp.sum(route_share[:, :, None] * picked, axis=1)).astype(jnp.bfloat16)
    return (mixer_out, moe_out)
```

```python
import functools

import jax
import jax.numpy as jnp
from jax import lax
from jax.experimental import pallas as pl
from jax.experimental.pallas import tpu as pltpu
from jax.sharding import PartitionSpec as P

MESH = pl.DeviceIdType.MESH
F32 = jnp.float32
BF16 = jnp.bfloat16
epsilon = 1e-06
lru_scale = 8.0

RING = 16
CORES = 2
EP = RING * CORES
SIDE = 4
ROWS = 256
D = 2048
LANE = 128
CAP = 32
SLOTS = EP * CAP
CHUNKS = 4
CH = SLOTS // CHUNKS
HALF = CH // 2
QUARTER = HALF // 2

NEAR = [0] + [s * d if s * d > -RING // 2 else RING // 2 for d in range(1, RING // 2 + 1) for s in (1, -1)][: RING - 1]
PLACE = {off % RING: at for at, off in enumerate(NEAR)}

ORDER = [
    ("R1", 0), ("mixA", 0), ("R2", 0), ("R1", 1), ("R3", 0), ("R2", 1), ("R1", 2), ("mixB", 0),
    ("R4", 0), ("R3", 1), ("R2", 2), ("R1", 3), ("mixC", 0), ("up", 0), ("H1", 0),
    ("R4", 1), ("R3", 2), ("R2", 3), ("H2", 0), ("up", 1), ("H1", 1),
    ("R4", 2), ("R3", 3), ("H3", 0), ("H2", 1), ("up", 2), ("H1", 2),
    ("R4", 3), ("H4", 0), ("H3", 1), ("H2", 2), ("up", 3), ("H1", 3), ("mixD", 0),
    ("down", 0), ("H4", 1), ("H3", 2), ("H2", 3),
    ("down", 1), ("H4", 2), ("H3", 3), ("down", 2), ("H4", 3), ("down", 3),
]


def softplus(v):
    e = jnp.exp(-jnp.abs(v))
    series = e * (1.0 - e * (1.0 / 2 - e * (1.0 / 3 - e * (1.0 / 4 - e * (1.0 / 5 - e / 6)))))
    return jnp.maximum(v, 0.0) + jnp.where(e < 0.03, series, jnp.log(1.0 + e))


def one_minus_exp(v):
    series = 1.0 + v / 8
    for n in (7, 6, 5, 4, 3, 2):
        series = 1.0 + v / n * series
    return jnp.where(v > -0.25, -v * series, 1.0 - jnp.exp(v))


def kernel(
    mix_in, moe_in, w_x, w_y, shift, w_gate, w_up, w_down,
    mix_gain, conv_taps, recur_w, input_w, logit, moe_gain, routes, weight,
    mixer_out, moe_out,
    mix_v, moe_v, win_v, shift_v, gu_v, down_v,
    c0, c1, sent, X, H, res, ret, ybr, xb, xcv, halo_out, halo_in, sa, sb, carry_out, carry_in,
    load_sem, ag_send, ag_recv, d_send, d_recv, r_send, r_recv, k_send, k_recv, h_sem,
):
    ep, tp = lax.axis_index("ep"), lax.axis_index("tp")
    z, core = ep // CORES, lax.rem(ep, CORES)
    y, x = tp // SIDE, lax.rem(tp, SIDE)

    def wrap(v, n):
        return lax.rem(v + 2 * n, n)

    east, west = wrap(x + 1, SIDE), wrap(x - 1, SIDE)
    north, south = wrap(y + 1, SIDE), wrap(y - 1, SIDE)
    plane = [(ep, y * SIDE + east), (ep, y * SIDE + west), (ep, north * SIDE + x), (ep, south * SIDE + x)]

    def peer(at, c):
        return wrap(z + NEAR[at], RING) * CORES + c

    loads = []
    for n, (src, dst) in enumerate([
        (moe_in, moe_v), (mix_in, mix_v), (w_x, win_v.at[:, :LANE]), (w_y, win_v.at[:, LANE:]), (shift, shift_v),
        (w_gate.at[0], gu_v.at[:, :LANE]), (w_up.at[0], gu_v.at[:, LANE:]), (w_down.at[0], down_v),
    ]):
        loads.append(pltpu.make_async_copy(src, dst, load_sem.at[n]))
        loads[-1].start()

    barrier = pltpu.get_barrier_semaphore()

    def greet(where):
        pl.semaphore_signal(barrier, inc=1, device_id=where, device_id_type=MESH)

    for where in plane:
        greet(where)
    greet((peer(0, 1 - core), tp))
    for at in range(1, RING):
        for c in range(CORES):
            greet((peer(at, c), tp))

    pending = []

    def launch(src, dst, ss, rs, where):
        copy = pltpu.make_async_remote_copy(
            src_ref=src, dst_ref=dst, send_sem=ss, recv_sem=rs, device_id=where, device_id_type=MESH
        )
        copy.start()
        pending.append(copy)
        return copy

    def normed(ref, gain, lanes):
        v = ref[...].astype(F32)
        scale = lax.rsqrt(jnp.sum(v * v, axis=1, keepdims=True) / D + epsilon)
        if lanes is not None:
            v = ref[:, lanes].astype(F32)
            return (v * scale * gain[:, lanes]).astype(BF16)
        return (v * scale * gain[...]).astype(BF16)

    lane_e = lax.broadcasted_iota(jnp.int32, (ROWS, LANE), 1)
    onehot = [jnp.where(routes[:, k : k + 1] == lane_e, 1.0, 0.0).astype(BF16) for k in range(2)]
    before = jnp.where(
        lax.broadcasted_iota(jnp.int32, (ROWS, ROWS), 1) < lax.broadcasted_iota(jnp.int32, (ROWS, ROWS), 0), 1.0, 0.0
    ).astype(BF16)
    rank = [jnp.dot(before, hot, preferred_element_type=F32) for hot in onehot]
    rank[1] = rank[1] + jnp.sum(onehot[0].astype(F32), axis=0, keepdims=True)
    lane_1 = lax.broadcasted_iota(jnp.int32, (1, LANE), 1)
    off = (lane_1 // CORES - z + 2 * RING) % RING
    at = jnp.where(off == 0, 0, jnp.where(off <= RING // 2, 2 * off - 1, 2 * (RING - off)))
    base = (CAP * (CORES * at + lane_1 % CORES)).astype(F32)
    slot_lane = lax.broadcasted_iota(jnp.int32, (ROWS, SLOTS), 1)
    for ref, hot, r in zip((c0, c1), onehot, rank):
        slot = jnp.sum(hot.astype(F32) * (r + base), axis=1, keepdims=True).astype(jnp.int32)
        ref[...] = jnp.where(slot_lane == slot, 1.0, 0.0).astype(BF16)

    loads[0].wait()
    own_lanes = pl.ds(pl.multiple_of(tp * LANE, LANE), LANE)
    own_rows = normed(moe_v, moe_gain, own_lanes)
    sent[...] = lax.dot_general(
        c0[...] + c1[...], own_rows, (((0,), (0,)), ((), ())), preferred_element_type=F32
    ).astype(BF16).reshape(EP, CAP, LANE)

    pl.semaphore_wait(barrier, len(plane) + EP - 1)

    def block(buf, p):
        return buf.at[y, x, pl.ds(pl.multiple_of(p * CAP, CAP), CAP)]

    def dispatch(at, c, where):
        place = PLACE[-NEAR[at] % RING] * CORES + core
        launch(sent.at[CORES * at + c], block(X, place), d_send.at[CORES * at + c], d_recv.at[place], (where, tp))

    dispatch(0, 1 - core, peer(0, 1 - core))
    for at in range(1, RING):
        for c in range(CORES):
            dispatch(at, c, peer(at, c))
    own = pl.ds(pl.multiple_of(core * CAP, CAP), CAP)
    X[y, x, own, :] = sent[core]

    def arrived(p, sem, buf_block):
        pltpu.make_async_remote_copy(
            src_ref=buf_block, dst_ref=buf_block, send_sem=sem.at[p], recv_sem=sem.at[p],
            device_id=(ep, tp), device_id_type=MESH,
        ).wait_recv()

    def await_dispatch(k):
        for p in range(k * CH // CAP, (k + 1) * CH // CAP):
            if p < CORES:
                if p == 0:
                    arrived(1 - core, d_recv, block(X, 1 - core))
            else:
                arrived(p, d_recv, block(X, p))

    bufs = {"R": X, "H": H}
    ways = {}

    def gather(kind, step, k):
        buf = bufs[kind]
        lo = k * CH
        xs, ys = pl.ds(lo, HALF), pl.ds(lo + HALF, HALF)
        xa, xz = pl.ds(lo, QUARTER), pl.ds(lo + QUARTER, QUARTER)
        ya, yz = pl.ds(lo + HALF, QUARTER), pl.ds(lo + HALF + QUARTER, QUARTER)
        if step == 1:
            if kind == "R":
                await_dispatch(k)
            views = [buf.at[y, x, xs], buf.at[y, x, xs], buf.at[y, x, ys], buf.at[y, x, ys]]
        elif step == 2:
            views = [buf.at[y, west, xa], buf.at[y, east, xz], buf.at[south, x, ya], buf.at[north, x, yz]]
        elif step == 3:
            views = [buf.at[:, x, ys], buf.at[:, x, ys], buf.at[y, :, xs], buf.at[y, :, xs]]
        else:
            views = [buf.at[:, west, ya], buf.at[:, east, yz], buf.at[south, :, xa], buf.at[north, :, xz]]
        if step == 3:
            for n in range(4):
                ways[kind, 2, k, n].wait_recv()
        for n in range(4):
            if step == 2 or step == 4:
                ways[kind, step - 1, k, n].wait_recv()
            slot = (("RH".index(kind) * CHUNKS + k) * 4 + step - 1) * 4 + n
            ways[kind, step, k, n] = launch(views[n], views[n], ag_send.at[slot], ag_recv.at[slot], plane[n])

    def all_blocks(buf, k):
        rows = pl.ds(k * CH, CH)
        return jnp.concatenate([buf[a, b, rows, :] for a in range(SIDE) for b in range(SIDE)], axis=1)

    def run_up(k):
        for n in range(4):
            ways["R", 4, k, n].wait_recv()
        if k == 0:
            loads[5].wait()
            loads[6].wait()
        both = jnp.dot(all_blocks(X, k), gu_v[...], preferred_element_type=F32)
        g, u = both[:, :LANE], both[:, LANE:]
        H[y, x, pl.ds(k * CH, CH), :] = (g * jax.nn.sigmoid(g) * u).astype(BF16)

    def run_down(k):
        for n in range(4):
            ways["H", 4, k, n].wait_recv()
        if k == 0:
            loads[7].wait()
        out = jnp.dot(all_blocks(H, k), down_v[...], preferred_element_type=F32).astype(BF16)
        first = k * CH // CAP
        res[pl.ds(first, CH // CAP)] = out.reshape(CH // CAP, CAP, LANE)

        def give(at, c, where):
            place = PLACE[-NEAR[at] % RING] * CORES + core
            launch(res.at[CORES * at + c], ret.at[place], r_send.at[CORES * at + c], r_recv.at[place], (where, tp))

        for p in range(first, first + CH // CAP):
            at, c = p // CORES, p % CORES
            if at == 0:
                if c == 0:
                    give(0, 1 - core, peer(0, 1 - core))
                    ret[core] = res[core]
            else:
                give(at, c, peer(at, c))

    def mix_a():
        loads[1].wait()
        loads[2].wait()
        loads[3].wait()
        rows = normed(mix_v, mix_gain, None)
        both = jnp.dot(rows, win_v[...], preferred_element_type=F32).astype(BF16)
        ybr[...] = both[:, LANE:]
        xb[pl.ds(8, ROWS), :] = both[:, :LANE].astype(F32)
        halo_out[...] = both[ROWS - 16 :, :LANE]
        ways["halo"] = launch(halo_out, halo_in, h_sem.at[0], h_sem.at[1], (wrap(ep + 1, EP), tp))

    def mix_b():
        ways["halo"].wait_recv()
        xb[pl.ds(0, 8), :] = jnp.where(ep > 0, halo_in[...].astype(F32)[8:], 0.0)
        conv = jnp.zeros((ROWS, LANE), F32)
        for k in range(4):
            conv = conv + conv_taps[k : k + 1, :] * xb[pl.ds(5 + k, ROWS), :]
        x_conv = conv.astype(BF16)
        xcv[...] = x_conv
        gate_a = jnp.dot(x_conv, recur_w[0], preferred_element_type=F32)
        gate_x = jnp.dot(x_conv, input_w[0], preferred_element_type=F32)
        loads[4].wait()
        log_decay = -lru_scale * jax.nn.sigmoid(gate_a) * softplus(-logit[...]) + shift_v[...]
        sa[...] = jnp.exp(log_decay)
        sb[...] = jnp.sqrt(one_minus_exp(2.0 * log_decay)) * jax.nn.sigmoid(gate_x) * x_conv.astype(F32)

    def mix_c():
        a, b = sa[...], sb[...]
        row = lax.broadcasted_iota(jnp.int32, (ROWS, LANE), 0)
        by = 1
        while by < ROWS:
            behind = row >= by
            b = jnp.where(behind, a * pltpu.roll(b, by, 0), 0.0) + b
            a = jnp.where(behind, pltpu.roll(a, by, 0), 1.0) * a
            by *= 2
        sa[...] = a
        sb[...] = b
        carry_out[0:1, :] = a[ROWS - 1 :, :]
        carry_out[1:2, :] = b[ROWS - 1 :, :]

        def tell(at, c):
            where = peer(at, c)
            launch(carry_out, carry_in.at[ep], k_send.at[CORES * at + c], k_recv.at[ep], (where, tp))

        tell(0, 1 - core)
        for at in range(1, RING):
            for c in range(CORES):
                tell(at, c)
        carry_in[ep] = carry_out[...]

    def mix_d():
        for at in range(RING):
            for c in range(CORES):
                if at == 0:
                    if c == 0:
                        who = peer(0, 1 - core)
                        arrived(who, k_recv, carry_in.at[who])
                else:
                    who = peer(at, c)
                    arrived(who, k_recv, carry_in.at[who])
        state = jnp.zeros((1, LANE), F32)
        for e in range(EP):
            pair = carry_in[e]
            state = jnp.where(e < ep, pair[0:1] * state + pair[1:2], state)
        lru = sb[...] + sa[...] * state
        mixer_out[...] = (lru * jax.nn.gelu(ybr[...].astype(F32), approximate=True)).astype(BF16)

    for what, k in ORDER:
        if what == "up":
            run_up(k)
        elif what == "down":
            run_down(k)
        elif what[:3] == "mix":
            {"A": mix_a, "B": mix_b, "C": mix_c, "D": mix_d}[what[3]]()
        else:
            gather(what[0], int(what[1]), k)

    arrived(1 - core, r_recv, ret.at[1 - core])
    for p in range(CORES, EP):
        arrived(p, r_recv, ret.at[p])
    back = ret[...].reshape(SLOTS, LANE)
    w = weight[...]
    total = w[:, 0:1] + w[:, 1:2]
    out = w[:, 0:1] / total * jnp.dot(c0[...], back, preferred_element_type=F32)
    out = out + w[:, 1:2] / total * jnp.dot(c1[...], back, preferred_element_type=F32)
    moe_out[...] = out.astype(BF16)
    for copy in pending:
        copy.wait_send()


def local(
    mix_in, mix_gain, w_in_x, w_in_y, conv_taps, recur_gate_w, input_gate_w, decay_logit, decay_shift,
    moe_in, moe_gain, routes, route_weight, expert_gate, expert_up, expert_down,
):
    anywhere = pl.BlockSpec(memory_space=pl.ANY)
    vmem = pl.BlockSpec(memory_space=pltpu.VMEM)
    dma = pltpu.SemaphoreType.DMA
    out = jax.ShapeDtypeStruct((ROWS, LANE), BF16)
    v = pltpu.VMEM
    return pl.pallas_call(
        kernel,
        out_shape=(out, out),
        in_specs=[anywhere] * 8 + [vmem] * 8,
        out_specs=(vmem, vmem),
        scratch_shapes=[
            v((ROWS, D), BF16), v((ROWS, D), BF16), v((D, 2 * LANE), BF16), v((ROWS, LANE), F32),
            v((D, 2 * LANE), BF16), v((D, LANE), BF16),
            v((ROWS, SLOTS), BF16), v((ROWS, SLOTS), BF16), v((EP, CAP, LANE), BF16),
            v((SIDE, SIDE, SLOTS, LANE), BF16), v((SIDE, SIDE, SLOTS, LANE), BF16),
            v((EP, CAP, LANE), BF16), v((EP, CAP, LANE), BF16),
            v((ROWS, LANE), BF16), v((ROWS + 8, LANE), F32), v((ROWS, LANE), BF16),
            v((16, LANE), BF16), v((16, LANE), BF16), v((ROWS, LANE), F32), v((ROWS, LANE), F32),
            v((2, LANE), F32), v((EP, 2, LANE), F32),
            dma((8,)), dma((2 * CHUNKS * 16,)), dma((2 * CHUNKS * 16,)), dma((EP,)), dma((EP,)),
            dma((EP,)), dma((EP,)), dma((EP,)), dma((EP,)), dma((2,)),
        ],
        compiler_params=pltpu.CompilerParams(
            collective_id=0, has_side_effects=True, vmem_limit_bytes=48 * 1024 * 1024
        ),
        name="mixer_and_experts",
    )(
        mix_in, moe_in, w_in_x, w_in_y, decay_shift, expert_gate, expert_up, expert_down,
        mix_gain.reshape(1, D), conv_taps, recur_gate_w, input_gate_w, decay_logit.reshape(1, LANE),
        moe_gain.reshape(1, D), routes, route_weight,
    )


def solution(mesh):
    placed = (
        P("ep", None),
        P(),
        P(None, "tp"),
        P(None, "tp"),
        P(None, "tp"),
        P("tp", None, None),
        P("tp", None, None),
        P("tp"),
        P("ep", "tp"),
        P("ep", None),
        P(),
        P("ep", None),
        P("ep", None),
        P("ep", None, "tp"),
        P("ep", None, "tp"),
        P("ep", None, "tp"),
    )
    return jax.shard_map(
        local, mesh=mesh, in_specs=placed, out_specs=(P("ep", "tp"), P("ep", "tp")), check_vma=False
    )
```

```python
import functools

import jax
import jax.numpy as jnp
from jax import lax
from jax.experimental import pallas as pl
from jax.experimental.pallas import tpu as pltpu
from jax.sharding import PartitionSpec as P

MESH = pl.DeviceIdType.MESH
F32 = jnp.float32
BF16 = jnp.bfloat16
epsilon = 1e-06
lru_scale = 8.0

RING = 16
CORES = 2
EP = RING * CORES
SIDE = 4
ROWS = 256
D = 2048
LANE = 128
CAP = 32
SLOTS = EP * CAP
CHUNKS = 4
CH = SLOTS // CHUNKS
HALF = CH // 2
QUARTER = HALF // 2

NEAR = [0, 1, -1, 2, 8, 7, -7, 6, -6, 5, -5, -4, 4, 3, -3, -2]
PLACE = {off % RING: at for at, off in enumerate(NEAR)}

ORDER = [
    ("R1", 0), ("mixA", 0), ("R2", 0), ("R3", 0), ("mixB", 0), ("R1", 1), ("R2", 1), ("R1", 2),
    ("R4", 0), ("R3", 1), ("R2", 2), ("R1", 3), ("mixC", 0), ("up", 0), ("H1", 0),
    ("R4", 1), ("R3", 2), ("R2", 3), ("H2", 0), ("up", 1), ("H1", 1),
    ("R4", 2), ("R3", 3), ("H3", 0), ("H2", 1), ("up", 2), ("H1", 2),
    ("R4", 3), ("H4", 0), ("H3", 1), ("H2", 2), ("up", 3), ("H1", 3), ("mixD", 0),
    ("down", 0), ("H4", 1), ("H3", 2), ("H2", 3),
    ("down", 1), ("H4", 2), ("H3", 3), ("down", 2), ("H4", 3), ("down", 3),
]


def softplus(v):
    e = jnp.exp(-jnp.abs(v))
    series = e * (1.0 - e * (1.0 / 2 - e * (1.0 / 3 - e * (1.0 / 4 - e * (1.0 / 5 - e / 6)))))
    return jnp.maximum(v, 0.0) + jnp.where(e < 0.03, series, jnp.log(1.0 + e))


def one_minus_exp(v):
    series = 1.0 + v / 8
    for n in (7, 6, 5, 4, 3, 2):
        series = 1.0 + v / n * series
    return jnp.where(v > -0.25, -v * series, 1.0 - jnp.exp(v))


def kernel(
    mix_in, moe_in, w_x, w_y, shift, w_gate, w_up, w_down,
    mix_gain, conv_taps, recur_w, input_w, logit, moe_gain, routes, weight,
    mixer_out, moe_out,
    mix_v, moe_v, win_v, shift_v, gu_v, down_v,
    mix_gain_v, conv_taps_v, recur_v, input_v, logit_v, moe_gain_v, routes_v, weight_v,
    c0, c1, sent, X, H, res, ret, ybr, xb, xcv, halo_out, halo_in, sa, sb, carry_out, carry_in,
    load_sem, ag_send, ag_recv, d_send, d_recv, r_send, r_recv, k_send, k_recv, h_sem,
):
    ep, tp = lax.axis_index("ep"), lax.axis_index("tp")
    z, core = ep // CORES, lax.rem(ep, CORES)
    y, x = tp // SIDE, lax.rem(tp, SIDE)

    def wrap(v, n):
        return lax.rem(v + 2 * n, n)

    east, west = wrap(x + 1, SIDE), wrap(x - 1, SIDE)
    north, south = wrap(y + 1, SIDE), wrap(y - 1, SIDE)
    plane = [(ep, y * SIDE + east), (ep, y * SIDE + west), (ep, north * SIDE + x), (ep, south * SIDE + x)]

    def peer(at, c):
        return wrap(z + NEAR[at], RING) * CORES + c

    loads = {}
    for n, (name, src, dst) in enumerate([
        ("routes", routes, routes_v), ("moe_gain", moe_gain, moe_gain_v), ("moe", moe_in, moe_v),
        ("mix_gain", mix_gain, mix_gain_v), ("mix", mix_in, mix_v),
        ("w_x", w_x, win_v.at[:, :LANE]), ("w_y", w_y, win_v.at[:, LANE:]),
        ("taps", conv_taps, conv_taps_v), ("recur", recur_w, recur_v), ("input", input_w, input_v),
        ("logit", logit, logit_v), ("shift", shift, shift_v),
        ("gate", w_gate.at[0], gu_v.at[:, :LANE]), ("up", w_up.at[0], gu_v.at[:, LANE:]), ("down", w_down.at[0], down_v),
        ("weight", weight, weight_v),
    ]):
        loads[name] = pltpu.make_async_copy(src, dst, load_sem.at[n])
        loads[name].start()

    def loaded(*names):
        for name in names:
            loads[name].wait()

    barrier = pltpu.get_barrier_semaphore()

    def greet(where):
        pl.semaphore_signal(barrier, inc=1, device_id=where, device_id_type=MESH)

    for where in plane:
        greet(where)
    greet((peer(0, 1 - core), tp))
    for at in range(1, RING):
        for c in range(CORES):
            greet((peer(at, c), tp))

    pending = []

    def launch(src, dst, ss, rs, where):
        copy = pltpu.make_async_remote_copy(
            src_ref=src, dst_ref=dst, send_sem=ss, recv_sem=rs, device_id=where, device_id_type=MESH
        )
        copy.start()
        pending.append(copy)
        return copy

    def normed(ref, gain, lanes):
        v = ref[...].astype(F32)
        scale = lax.rsqrt(jnp.sum(v * v, axis=1, keepdims=True) / D + epsilon)
        if lanes is not None:
            v = ref[:, lanes].astype(F32)
            return (v * scale * gain[:, lanes]).astype(BF16)
        return (v * scale * gain[...]).astype(BF16)

    def columns(ref):
        flat = ref[...].astype(F32)
        return jnp.transpose(jnp.concatenate([flat] * 4, axis=0))

    lane_e = lax.broadcasted_iota(jnp.int32, (ROWS, LANE), 1)
    loaded("routes")
    chosen = columns(routes_v).astype(jnp.int32)
    onehot = [jnp.where(chosen[:, k : k + 1] == lane_e, 1.0, 0.0).astype(BF16) for k in range(2)]
    before = jnp.where(
        lax.broadcasted_iota(jnp.int32, (ROWS, ROWS), 1) < lax.broadcasted_iota(jnp.int32, (ROWS, ROWS), 0), 1.0, 0.0
    ).astype(BF16)
    rank = [jnp.dot(before, hot, preferred_element_type=F32) for hot in onehot]
    rank[1] = rank[1] + jnp.sum(onehot[0].astype(F32), axis=0, keepdims=True)
    lane_1 = lax.broadcasted_iota(jnp.int32, (1, LANE), 1)
    off = (lane_1 // CORES - z + 2 * RING) % RING
    at = jnp.zeros((1, LANE), jnp.int32)
    for n in range(1, RING):
        at = jnp.where(off == NEAR[n] % RING, n, at)
    base = (CAP * (CORES * at + lane_1 % CORES)).astype(F32)
    slot_lane = lax.broadcasted_iota(jnp.int32, (ROWS, SLOTS), 1)
    for ref, hot, r in zip((c0, c1), onehot, rank):
        slot = jnp.sum(hot.astype(F32) * (r + base), axis=1, keepdims=True).astype(jnp.int32)
        ref[...] = jnp.where(slot_lane == slot, 1.0, 0.0).astype(BF16)

    loaded("moe", "moe_gain")
    own_lanes = pl.ds(pl.multiple_of(tp * LANE, LANE), LANE)
    own_rows = normed(moe_v, moe_gain_v, own_lanes)
    sent[...] = lax.dot_general(
        c0[...] + c1[...], own_rows, (((0,), (0,)), ((), ())), preferred_element_type=F32
    ).astype(BF16).reshape(EP, CAP, LANE)

    with jax.named_scope("barrier"):
        pl.semaphore_wait(barrier, len(plane) + EP - 1)

    def block(buf, p):
        return buf.at[y, x, pl.ds(pl.multiple_of(p * CAP, CAP), CAP)]

    def dispatch(at, c, where):
        place = PLACE[-NEAR[at] % RING] * CORES + core
        launch(sent.at[CORES * at + c], block(X, place), d_send.at[CORES * at + c], d_recv.at[place], (where, tp))

    dispatch(0, 1 - core, peer(0, 1 - core))
    for at in range(1, RING):
        for c in range(CORES):
            dispatch(at, c, peer(at, c))
    own = pl.ds(pl.multiple_of(core * CAP, CAP), CAP)
    X[y, x, own, :] = sent[core]

    def arrived(p, sem, buf_block):
        pltpu.make_async_remote_copy(
            src_ref=buf_block, dst_ref=buf_block, send_sem=sem.at[p], recv_sem=sem.at[p],
            device_id=(ep, tp), device_id_type=MESH,
        ).wait_recv()

    def await_dispatch(k):
        for p in range(k * CH // CAP, (k + 1) * CH // CAP):
            if p < CORES:
                if p == 0:
                    arrived(1 - core, d_recv, block(X, 1 - core))
            else:
                arrived(p, d_recv, block(X, p))

    bufs = {"R": X, "H": H}
    ways = {}

    def gather(kind, step, k):
        buf = bufs[kind]
        lo = k * CH
        xs, ys = pl.ds(lo, HALF), pl.ds(lo + HALF, HALF)
        xa, xz = pl.ds(lo, QUARTER), pl.ds(lo + QUARTER, QUARTER)
        ya, yz = pl.ds(lo + HALF, QUARTER), pl.ds(lo + HALF + QUARTER, QUARTER)
        if step == 1:
            if kind == "R":
                await_dispatch(k)
            views = [buf.at[y, x, xs], buf.at[y, x, xs], buf.at[y, x, ys], buf.at[y, x, ys]]
        elif step == 2:
            views = [buf.at[y, west, xa], buf.at[y, east, xz], buf.at[south, x, ya], buf.at[north, x, yz]]
        elif step == 3:
            views = [buf.at[:, x, ys], buf.at[:, x, ys], buf.at[y, :, xs], buf.at[y, :, xs]]
        else:
            views = [buf.at[:, west, ya], buf.at[:, east, yz], buf.at[south, :, xa], buf.at[north, :, xz]]
        if step == 3:
            for n in range(4):
                ways[kind, 2, k, n].wait_recv()
        for n in range(4):
            if step == 2 or step == 4:
                ways[kind, step - 1, k, n].wait_recv()
            slot = (("RH".index(kind) * CHUNKS + k) * 4 + step - 1) * 4 + n
            ways[kind, step, k, n] = launch(views[n], views[n], ag_send.at[slot], ag_recv.at[slot], plane[n])

    def all_blocks(buf, k):
        rows = pl.ds(k * CH, CH)
        return jnp.concatenate([buf[a, b, rows, :] for a in range(SIDE) for b in range(SIDE)], axis=1)

    def run_up(k):
        for n in range(4):
            ways["R", 4, k, n].wait_recv()
        if k == 0:
            loaded("gate", "up")
        both = jnp.dot(all_blocks(X, k), gu_v[...], preferred_element_type=F32)
        g, u = both[:, :LANE], both[:, LANE:]
        H[y, x, pl.ds(k * CH, CH), :] = (g * jax.nn.sigmoid(g) * u).astype(BF16)

    def run_down(k):
        for n in range(4):
            ways["H", 4, k, n].wait_recv()
        if k == 0:
            loaded("down")
        out = jnp.dot(all_blocks(H, k), down_v[...], preferred_element_type=F32).astype(BF16)
        first = k * CH // CAP
        res[pl.ds(first, CH // CAP)] = out.reshape(CH // CAP, CAP, LANE)

        def give(at, c, where):
            place = PLACE[-NEAR[at] % RING] * CORES + core
            launch(res.at[CORES * at + c], ret.at[place], r_send.at[CORES * at + c], r_recv.at[place], (where, tp))

        for p in range(first, first + CH // CAP):
            at, c = p // CORES, p % CORES
            if at == 0:
                if c == 0:
                    give(0, 1 - core, peer(0, 1 - core))
                    ret[core] = res[core]
            else:
                give(at, c, peer(at, c))

    def mix_a():
        loaded("mix", "mix_gain", "w_x", "w_y")
        rows = normed(mix_v, mix_gain_v, None)
        both = jnp.dot(rows, win_v[...], preferred_element_type=F32).astype(BF16)
        ybr[...] = both[:, LANE:]
        xb[pl.ds(8, ROWS), :] = both[:, :LANE].astype(F32)
        halo_out[...] = both[ROWS - 16 :, :LANE]
        ways["halo"] = launch(halo_out, halo_in, h_sem.at[0], h_sem.at[1], (wrap(ep + 1, EP), tp))

    def mix_b():
        ways["halo"].wait_recv()
        loaded("taps", "recur", "input", "logit", "shift")
        xb[pl.ds(0, 8), :] = jnp.where(ep > 0, halo_in[...].astype(F32)[8:], 0.0)
        conv = jnp.zeros((ROWS, LANE), F32)
        for k in range(4):
            conv = conv + conv_taps_v[k : k + 1, :] * xb[pl.ds(5 + k, ROWS), :]
        x_conv = conv.astype(BF16)
        xcv[...] = x_conv
        gate_a = jnp.dot(x_conv, recur_v[0], preferred_element_type=F32)
        gate_x = jnp.dot(x_conv, input_v[0], preferred_element_type=F32)
        log_decay = -lru_scale * jax.nn.sigmoid(gate_a) * softplus(-logit_v[...]) + shift_v[...]
        sa[...] = jnp.exp(log_decay)
        sb[...] = jnp.sqrt(one_minus_exp(2.0 * log_decay)) * jax.nn.sigmoid(gate_x) * x_conv.astype(F32)

    def mix_c():
        a, b = sa[...], sb[...]
        row = lax.broadcasted_iota(jnp.int32, (ROWS, LANE), 0)
        by = 1
        while by < ROWS:
            behind = row >= by
            b = jnp.where(behind, a * pltpu.roll(b, by, 0), 0.0) + b
            a = jnp.where(behind, pltpu.roll(a, by, 0), 1.0) * a
            by *= 2
        sa[...] = a
        sb[...] = b
        carry_out[0:1, :] = a[ROWS - 1 :, :]
        carry_out[1:2, :] = b[ROWS - 1 :, :]

        def tell(at, c):
            where = peer(at, c)
            launch(carry_out, carry_in.at[ep], k_send.at[CORES * at + c], k_recv.at[ep], (where, tp))

        tell(0, 1 - core)
        for at in range(1, RING):
            for c in range(CORES):
                tell(at, c)
        carry_in[ep] = carry_out[...]

    def mix_d():
        for at in range(RING):
            for c in range(CORES):
                if at == 0:
                    if c == 0:
                        who = peer(0, 1 - core)
                        arrived(who, k_recv, carry_in.at[who])
                else:
                    who = peer(at, c)
                    arrived(who, k_recv, carry_in.at[who])
        state = jnp.zeros((1, LANE), F32)
        for e in range(EP):
            pair = carry_in[e]
            state = jnp.where(e < ep, pair[0:1] * state + pair[1:2], state)
        lru = sb[...] + sa[...] * state
        mixer_out[...] = (lru * jax.nn.gelu(ybr[...].astype(F32), approximate=True)).astype(BF16)

    for what, k in ORDER:
        with jax.named_scope(f"{what}_{k}"):
            if what == "up":
                run_up(k)
            elif what == "down":
                run_down(k)
            elif what[:3] == "mix":
                {"A": mix_a, "B": mix_b, "C": mix_c, "D": mix_d}[what[3]]()
            else:
                gather(what[0], int(what[1]), k)

    with jax.named_scope("back"):
        arrived(1 - core, r_recv, ret.at[1 - core])
        for p in range(CORES, EP):
            arrived(p, r_recv, ret.at[p])
    back = ret[...].reshape(SLOTS, LANE)
    loaded("weight")
    w = columns(weight_v)
    total = w[:, 0:1] + w[:, 1:2]
    out = w[:, 0:1] / total * jnp.dot(c0[...], back, preferred_element_type=F32)
    out = out + w[:, 1:2] / total * jnp.dot(c1[...], back, preferred_element_type=F32)
    moe_out[...] = out.astype(BF16)
    with jax.named_scope("sends"):
        for copy in pending:
            copy.wait_send()


def local(
    mix_in, mix_gain, w_in_x, w_in_y, conv_taps, recur_gate_w, input_gate_w, decay_logit, decay_shift,
    moe_in, moe_gain, routes, route_weight, expert_gate, expert_up, expert_down,
):
    hbm = pl.BlockSpec(memory_space=pltpu.HBM)
    vmem = pl.BlockSpec(memory_space=pltpu.VMEM)
    dma = pltpu.SemaphoreType.DMA
    out = jax.ShapeDtypeStruct((ROWS, LANE), BF16)
    v = pltpu.VMEM
    return pl.pallas_call(
        kernel,
        out_shape=(out, out),
        in_specs=[hbm] * 16,
        out_specs=(vmem, vmem),
        scratch_shapes=[
            v((ROWS, D), BF16), v((ROWS, D), BF16), v((D, 2 * LANE), BF16), v((ROWS, LANE), F32),
            v((D, 2 * LANE), BF16), v((D, LANE), BF16),
            v((1, D), F32), v((4, LANE), F32), v((1, LANE, LANE), BF16), v((1, LANE, LANE), BF16), v((1, LANE), F32),
            v((1, D), F32), v((2, ROWS), jnp.int32), v((2, ROWS), F32),
            v((ROWS, SLOTS), BF16), v((ROWS, SLOTS), BF16), v((EP, CAP, LANE), BF16),
            v((SIDE, SIDE, SLOTS, LANE), BF16), v((SIDE, SIDE, SLOTS, LANE), BF16),
            v((EP, CAP, LANE), BF16), v((EP, CAP, LANE), BF16),
            v((ROWS, LANE), BF16), v((ROWS + 8, LANE), F32), v((ROWS, LANE), BF16),
            v((16, LANE), BF16), v((16, LANE), BF16), v((ROWS, LANE), F32), v((ROWS, LANE), F32),
            v((2, LANE), F32), v((EP, 2, LANE), F32),
            dma((16,)), dma((2 * CHUNKS * 16,)), dma((2 * CHUNKS * 16,)), dma((EP,)), dma((EP,)),
            dma((EP,)), dma((EP,)), dma((EP,)), dma((EP,)), dma((2,)),
        ],
        compiler_params=pltpu.CompilerParams(
            collective_id=0, has_side_effects=True, vmem_limit_bytes=67043328
        ),
        name="mixer_and_experts",
    )(
        mix_in, moe_in, w_in_x, w_in_y, decay_shift, expert_gate, expert_up, expert_down,
        mix_gain.reshape(1, D), conv_taps, recur_gate_w, input_gate_w, decay_logit.reshape(1, LANE),
        moe_gain.reshape(1, D), routes.T, route_weight.T,
    )


def solution(mesh):
    placed = (
        P("ep", None),
        P(),
        P(None, "tp"),
        P(None, "tp"),
        P(None, "tp"),
        P("tp", None, None),
        P("tp", None, None),
        P("tp"),
        P("ep", "tp"),
        P("ep", None),
        P(),
        P("ep", None),
        P("ep", None),
        P("ep", None, "tp"),
        P("ep", None, "tp"),
        P("ep", None, "tp"),
    )
    return jax.shard_map(
        local, mesh=mesh, in_specs=placed, out_specs=(P("ep", "tp"), P("ep", "tp")), check_vma=False
    )
```

```python
import functools

import jax
import jax.numpy as jnp
from jax import lax
from jax.experimental import pallas as pl
from jax.experimental.pallas import tpu as pltpu
from jax.sharding import PartitionSpec as P

MESH = pl.DeviceIdType.MESH
F32 = jnp.float32
BF16 = jnp.bfloat16
epsilon = 1e-06
lru_scale = 8.0

RING = 16
CORES = 2
EP = RING * CORES
SIDE = 4
ROWS = 256
D = 2048
LANE = 128
CAP = 32
SLOTS = EP * CAP
CHUNKS = 4
CH = SLOTS // CHUNKS
QROWS = CH // SIDE
PIECES = 8
WROWS = D // PIECES

XROWS = [128, 128, 128, 128]

NEAR = [0, 1, -1, 2, -7, 7, 6, 8, 5, -6, -4, -5, 4, -3, 3, -2]
PLACE = {off % RING: at for at, off in enumerate(NEAR)}

ORDER = [
    "MA0", "Y10", "X10", "W16", "Y20", "X20", "Y30", "W21", "X30", "MB0", "MC0", "Y11", "X11", "Y40", "X40", "Y12",
    "X12", "Y21", "X21", "Y22", "Y31", "X22", "Y13", "X13", "X31", "Y32", "Y23", "Y41", "X32", "X23", "UP0", "X41",
    "MD0", "Y33", "Y42", "W17", "W20", "X42", "X33", "B10", "UP1", "Y43", "W23", "B20", "UP2", "X43", "W22", "B11",
    "B12", "UP3", "B21", "DN0", "B13", "B22", "DN1", "B23", "DN2", "DN3",
]
EARLY = 6


def softplus(v):
    e = jnp.exp(-jnp.abs(v))
    series = e * (1.0 - e * (1.0 / 2 - e * (1.0 / 3 - e * (1.0 / 4 - e * (1.0 / 5 - e / 6)))))
    return jnp.maximum(v, 0.0) + jnp.where(e < 0.03, series, jnp.log(1.0 + e))


def one_minus_exp(v):
    series = 1.0 + v / 8
    for n in (7, 6, 5, 4, 3, 2):
        series = 1.0 + v / n * series
    return jnp.where(v > -0.25, -v * series, 1.0 - jnp.exp(v))


def kernel(
    mix_in, moe_in, w_x, w_y, shift, w_gate, w_up, w_down,
    mix_gain, conv_taps, recur_w, input_w, logit, moe_gain, routes, weight,
    mixer_out, moe_out,
    mix_v, moe_v, win_v, shift_v, gu_v, wd,
    mix_gain_v, conv_taps_v, recur_v, input_v, logit_v, moe_gain_v, routes_v, weight_v,
    c0, c1, sent, X, hown, H, res, ret, ybr, xb, xcv, halo_out, halo_in, sa, sb, carry_out, carry_in,
    load_sem, x_send, x_recv, b_send, b_recv, a_send, a_recv, w_send, w_recv,
    d_send, d_recv, r_send, r_recv, k_send, k_recv, h_sem,
):
    ep, tp = lax.axis_index("ep"), lax.axis_index("tp")
    z, core = ep // CORES, lax.rem(ep, CORES)
    y, x = tp // SIDE, lax.rem(tp, SIDE)

    def wrap(v, n):
        return lax.rem(v + 2 * n, n)

    east, west = wrap(x + 1, SIDE), wrap(x - 1, SIDE)
    north, south = wrap(y + 1, SIDE), wrap(y - 1, SIDE)
    across = wrap(x + 2, SIDE)
    plane = [(ep, y * SIDE + east), (ep, y * SIDE + west), (ep, north * SIDE + x), (ep, south * SIDE + x)]
    row = [plane[0], plane[1], (ep, y * SIDE + across)]

    def by_x(values, of):
        got = values[0]
        for n in range(1, SIDE):
            got = jnp.where(of == n, values[n], got)
        return got

    def offset(k, of):
        return by_x(NEAR[SIDE * k : SIDE * (k + 1)], of)

    def lanes(n):
        return pl.ds(pl.multiple_of(n * LANE, LANE), LANE)

    def peer(at, c):
        return wrap(z + NEAR[at], RING) * CORES + c

    loads = {}
    for n, (name, src, dst) in enumerate([
        ("routes", routes, routes_v), ("down", w_down.at[0], wd.at[:, lanes(x)]), ("moe_gain", moe_gain, moe_gain_v), ("moe", moe_in, moe_v),
        ("mix_gain", mix_gain, mix_gain_v), ("mix", mix_in, mix_v),
        ("w_x", w_x, win_v.at[:, :LANE]), ("w_y", w_y, win_v.at[:, LANE:]),
        ("taps", conv_taps, conv_taps_v), ("recur", recur_w, recur_v), ("input", input_w, input_v),
        ("logit", logit, logit_v), ("shift", shift, shift_v),
        ("gate", w_gate.at[0], gu_v.at[:, :LANE]), ("up", w_up.at[0], gu_v.at[:, LANE:]),
        ("weight", weight, weight_v),
    ]):
        loads[name] = pltpu.make_async_copy(src, dst, load_sem.at[n])
        loads[name].start()

    def loaded(*names):
        for name in names:
            loads[name].wait()

    barrier = pltpu.get_barrier_semaphore()

    def greet(where):
        pl.semaphore_signal(barrier, inc=1, device_id=where, device_id_type=MESH)

    for where in plane + row[2:]:
        greet(where)
    greet((peer(0, 1 - core), tp))
    for at in range(1, RING):
        for c in range(CORES):
            greet((peer(at, c), tp))
    for k in range(CHUNKS):
        for by in range(1, SIDE):
            other = wrap(x + by, SIDE)
            for c in range(CORES):
                greet((wrap(z + offset(k, x), RING) * CORES + c, y * SIDE + other))
                greet((wrap(z - offset(k, other), RING) * CORES + c, y * SIDE + other))
    greeted = len(plane) + 1 + EP - 1 + 2 * CHUNKS * (SIDE - 1) * CORES

    pending = []

    def launch(src, dst, ss, rs, where):
        copy = pltpu.make_async_remote_copy(
            src_ref=src, dst_ref=dst, send_sem=ss, recv_sem=rs, device_id=where, device_id_type=MESH
        )
        copy.start()
        pending.append(copy)
        return copy

    def normed(ref, gain, lanes):
        v = ref[...].astype(F32)
        scale = lax.rsqrt(jnp.sum(v * v, axis=1, keepdims=True) / D + epsilon)
        if lanes is not None:
            v = ref[:, lanes].astype(F32)
            return (v * scale * gain[:, lanes]).astype(BF16)
        return (v * scale * gain[...]).astype(BF16)

    def columns(ref):
        flat = ref[...].astype(F32)
        return jnp.transpose(jnp.concatenate([flat] * 4, axis=0))

    lane_e = lax.broadcasted_iota(jnp.int32, (ROWS, LANE), 1)
    loaded("routes")
    chosen = columns(routes_v).astype(jnp.int32)
    onehot = [jnp.where(chosen[:, k : k + 1] == lane_e, 1.0, 0.0).astype(BF16) for k in range(2)]
    before = jnp.where(
        lax.broadcasted_iota(jnp.int32, (ROWS, ROWS), 1) < lax.broadcasted_iota(jnp.int32, (ROWS, ROWS), 0), 1.0, 0.0
    ).astype(BF16)
    rank = [jnp.dot(before, hot, preferred_element_type=F32) for hot in onehot]
    rank[1] = rank[1] + jnp.sum(onehot[0].astype(F32), axis=0, keepdims=True)
    lane_1 = lax.broadcasted_iota(jnp.int32, (1, LANE), 1)
    off = (lane_1 // CORES - z + 2 * RING) % RING
    at = jnp.zeros((1, LANE), jnp.int32)
    for n in range(1, RING):
        at = jnp.where(off == NEAR[n] % RING, n, at)
    base = (CAP * (CORES * at + lane_1 % CORES)).astype(F32)
    slot_lane = lax.broadcasted_iota(jnp.int32, (ROWS, SLOTS), 1)
    for ref, hot, r in zip((c0, c1), onehot, rank):
        slot = jnp.sum(hot.astype(F32) * (r + base), axis=1, keepdims=True).astype(jnp.int32)
        ref[...] = jnp.where(slot_lane == slot, 1.0, 0.0).astype(BF16)

    with jax.named_scope("barrier"):
        pl.semaphore_wait(barrier, greeted)
    loaded("down")
    ways = {}

    def weights(step, q):
        if step == 1:
            views = [(wd.at[pl.ds(q * WROWS, WROWS), lanes(x)], q)] * 2
        else:
            ways["W", 1, q, 0].wait_recv()
            ways["W", 1, q + PIECES // 2, 1].wait_recv()
            views = [
                (wd.at[pl.ds(q * WROWS, WROWS), lanes(west)], PIECES + q),
                (wd.at[pl.ds((q + PIECES // 2) * WROWS, WROWS), lanes(east)], PIECES + q),
            ]
        for n, (view, slot) in enumerate(views):
            ways["W", step, q, n] = launch(view, view, w_send.at[2 * slot + n], w_recv.at[2 * slot + n], row[n])

    for q in range(EARLY):
        weights(1, q)

    loaded("moe", "moe_gain")
    own_rows = normed(moe_v, moe_gain_v, lanes(tp))
    sent[...] = lax.dot_general(
        c0[...] + c1[...], own_rows, (((0,), (0,)), ((), ())), preferred_element_type=F32
    ).astype(BF16).reshape(EP, CAP, LANE)

    def block(buf, p):
        return buf.at[y, x, pl.ds(pl.multiple_of(p * CAP, CAP), CAP)]

    def dispatch(at, c):
        local = CORES * PLACE[-NEAR[at] % RING] + c
        place = CORES * at + core
        where = wrap(z - NEAR[at], RING) * CORES + c
        launch(sent.at[local], block(X, place), d_send.at[local], d_recv.at[place], (where, tp))

    dispatch(0, 1 - core)
    for at in range(1, RING):
        for c in range(CORES):
            dispatch(at, c)
    own = pl.ds(pl.multiple_of(core * CAP, CAP), CAP)
    X[y, x, own, :] = sent[core]

    def arrived(p, sem, ref):
        pltpu.make_async_remote_copy(
            src_ref=ref, dst_ref=ref, send_sem=sem.at[p], recv_sem=sem.at[p],
            device_id=(ep, tp), device_id_type=MESH,
        ).wait_recv()

    def await_dispatch(k):
        if ("in", k) in ways:
            return
        ways["in", k] = None
        for p in range(k * CH // CAP, (k + 1) * CH // CAP):
            if p >= CORES:
                arrived(p, d_recv, block(X, p))
            elif p == 0:
                arrived(1 - core, d_recv, block(X, 1 - core))

    def gather(part, step, k):
        lo, size = k * CH, XROWS[k]
        if part == "Y":
            lo, size = lo + size, CH - size
        full, first, second = pl.ds(lo, size), pl.ds(lo, size // 2), pl.ds(lo + size // 2, size // 2)
        along_x = (part == "X") == (step < 3)
        if step == 1:
            await_dispatch(k)
            views = [X.at[y, x, full]] * 2
        elif step == 2 and along_x:
            views = [X.at[y, west, first], X.at[y, east, second]]
        elif step == 2:
            views = [X.at[south, x, first], X.at[north, x, second]]
        elif step == 3 and along_x:
            views = [X.at[:, x, full]] * 2
        elif step == 3:
            views = [X.at[y, :, full]] * 2
        elif along_x:
            views = [X.at[:, west, first], X.at[:, east, second]]
        else:
            views = [X.at[south, :, first], X.at[north, :, second]]
        if step == 3:
            for n in range(2):
                ways[part, 2, k, n].wait_recv()
        for n in range(2):
            if step == 2 or step == 4:
                ways[part, step - 1, k, n].wait_recv()
            slot = ((("XY".index(part) * CHUNKS) + k) * 4 + step - 1) * 2 + n
            ways[part, step, k, n] = launch(
                views[n], views[n], x_send.at[slot], x_recv.at[slot], plane[n if along_x else 2 + n]
            )

    def all_blocks(buf, rows):
        return jnp.concatenate([buf[a, b, rows, :] for a in range(SIDE) for b in range(SIDE)], axis=1)

    def quarter(k, n):
        return pl.ds(pl.multiple_of(k * CH + n * QROWS, QROWS), QROWS)

    def run_up(k):
        for part in "XY":
            for n in range(2):
                ways[part, 4, k, n].wait_recv()
        if k == 0:
            loaded("gate", "up")
        both = jnp.dot(all_blocks(X, pl.ds(k * CH, CH)), gu_v[...], preferred_element_type=F32)
        g, u = both[:, :LANE], both[:, LANE:]
        hown[pl.ds(k * CH, CH), :] = (g * jax.nn.sigmoid(g) * u).astype(BF16)
        mine = pl.ds(k * QROWS, QROWS)
        for n, who in enumerate((east, west, across)):
            slot = 3 * k + n
            ways["A", k, n] = launch(hown.at[quarter(k, who)], H.at[y, x, mine], a_send.at[slot], a_recv.at[slot], row[n])
        H[y, x, mine, :] = hown[quarter(k, x), :]

    def spread(step, k):
        slot = 4 * k + 2 * (step - 1)
        lo = k * QROWS
        if step == 1:
            for n, who in enumerate((west, east, across)):
                ways["A", k, n].wait_recv()
            views = [H.at[y, :, pl.ds(lo, QROWS)]] * 2
        else:
            views = [H.at[south, :, pl.ds(lo, QROWS // 2)], H.at[north, :, pl.ds(lo + QROWS // 2, QROWS // 2)]]
        for n in range(2):
            if step == 2:
                ways["B", 1, k, n].wait_recv()
            ways["B", step, k, n] = launch(views[n], views[n], b_send.at[slot + n], b_recv.at[slot + n], plane[2 + n])

    def give(k, c, by, act):
        other = wrap(x + by, SIDE)
        off = offset(k, x)
        place = by_x([PLACE[-v % RING] for v in NEAR[SIDE * k : SIDE * (k + 1)]], x) * CORES + core
        slot = (k * CORES + c) * SIDE + by
        copy = pltpu.make_async_remote_copy(
            src_ref=res.at[k * CORES + c, other], dst_ref=ret.at[place], send_sem=r_send.at[slot], recv_sem=r_recv.at[place],
            device_id=(wrap(z + off, RING) * CORES + c, y * SIDE + other), device_id_type=MESH,
        )
        if k == 0 and by == 0:
            stays = jnp.logical_and(x == 0, core == c)

            @pl.when(jnp.logical_not(stays))
            def _():
                act(copy)

            if act is starts:

                @pl.when(stays)
                def _():
                    ret[core] = res[c, 0]

        else:
            act(copy)

    def starts(copy):
        copy.start()

    def run_down(k):
        for n in range(2):
            ways["B", 2, k, n].wait_recv()
        if k == 0:
            for q in range(PIECES // 2):
                ways["W", 1, q, 1].wait_recv()
                ways["W", 1, q + PIECES // 2, 0].wait_recv()
                ways["W", 2, q, 0].wait_recv()
                ways["W", 2, q, 1].wait_recv()
        out = jnp.dot(all_blocks(H, pl.ds(k * QROWS, QROWS)), wd[...], preferred_element_type=F32).astype(BF16)
        for n in range(SIDE):
            for c in range(CORES):
                res[k * CORES + c, n] = out[c * CAP : (c + 1) * CAP, n * LANE : (n + 1) * LANE]
        for by in range(SIDE):
            for c in range(CORES):
                give(k, c, by, starts)

    def mix_a():
        loaded("mix", "mix_gain", "w_x", "w_y")
        rows = normed(mix_v, mix_gain_v, None)
        both = jnp.dot(rows, win_v[...], preferred_element_type=F32).astype(BF16)
        ybr[...] = both[:, LANE:]
        xb[pl.ds(8, ROWS), :] = both[:, :LANE].astype(F32)
        halo_out[...] = both[ROWS - 16 :, :LANE]
        ways["halo"] = launch(halo_out, halo_in, h_sem.at[0], h_sem.at[1], (wrap(ep + 1, EP), tp))

    def mix_b():
        ways["halo"].wait_recv()
        loaded("taps", "recur", "input", "logit", "shift")
        xb[pl.ds(0, 8), :] = jnp.where(ep > 0, halo_in[...].astype(F32)[8:], 0.0)
        conv = jnp.zeros((ROWS, LANE), F32)
        for k in range(4):
            conv = conv + conv_taps_v[k : k + 1, :] * xb[pl.ds(5 + k, ROWS), :]
        x_conv = conv.astype(BF16)
        xcv[...] = x_conv
        gate_a = jnp.dot(x_conv, recur_v[0], preferred_element_type=F32)
        gate_x = jnp.dot(x_conv, input_v[0], preferred_element_type=F32)
        log_decay = -lru_scale * jax.nn.sigmoid(gate_a) * softplus(-logit_v[...]) + shift_v[...]
        sa[...] = jnp.exp(log_decay)
        sb[...] = jnp.sqrt(one_minus_exp(2.0 * log_decay)) * jax.nn.sigmoid(gate_x) * x_conv.astype(F32)

    def mix_c():
        a, b = sa[...], sb[...]
        row = lax.broadcasted_iota(jnp.int32, (ROWS, LANE), 0)
        by = 1
        while by < ROWS:
            behind = row >= by
            b = jnp.where(behind, a * pltpu.roll(b, by, 0), 0.0) + b
            a = jnp.where(behind, pltpu.roll(a, by, 0), 1.0) * a
            by *= 2
        sa[...] = a
        sb[...] = b
        carry_out[0:1, :] = a[ROWS - 1 :, :]
        carry_out[1:2, :] = b[ROWS - 1 :, :]

        def tell(at, c):
            where = peer(at, c)
            launch(carry_out, carry_in.at[ep], k_send.at[CORES * at + c], k_recv.at[ep], (where, tp))

        tell(0, 1 - core)
        for at in range(1, RING):
            for c in range(CORES):
                tell(at, c)
        carry_in[ep] = carry_out[...]

    def mix_d():
        for at in range(RING):
            for c in range(CORES):
                if at > 0 or c == 0:
                    who = peer(at, c) if at else peer(0, 1 - core)
                    arrived(who, k_recv, carry_in.at[who])
        state = jnp.zeros((1, LANE), F32)
        for e in range(EP):
            pair = carry_in[e]
            state = jnp.where(e < ep, pair[0:1] * state + pair[1:2], state)
        lru = sb[...] + sa[...] * state
        mixer_out[...] = (lru * jax.nn.gelu(ybr[...].astype(F32), approximate=True)).astype(BF16)

    for item in ORDER:
        what, k = item[:-1], int(item[-1])
        with jax.named_scope(f"{what}_{k}"):
            if what == "UP":
                run_up(k)
            elif what == "DN":
                run_down(k)
            elif what[0] == "M":
                {"A": mix_a, "B": mix_b, "C": mix_c, "D": mix_d}[what[1]]()
            elif what[0] == "W":
                weights(int(what[1]), k)
            elif what[0] == "B":
                spread(int(what[1]), k)
            else:
                gather(what[0], int(what[1]), k)

    with jax.named_scope("back"):
        arrived(1 - core, r_recv, ret.at[1 - core])
        for p in range(CORES, EP):
            arrived(p, r_recv, ret.at[p])

        @pl.when(x != 0)
        def _():
            arrived(core, r_recv, ret.at[core])

    back = ret[...].reshape(SLOTS, LANE)
    loaded("weight")
    w = columns(weight_v)
    total = w[:, 0:1] + w[:, 1:2]
    out = w[:, 0:1] / total * jnp.dot(c0[...], back, preferred_element_type=F32)
    out = out + w[:, 1:2] / total * jnp.dot(c1[...], back, preferred_element_type=F32)
    moe_out[...] = out.astype(BF16)
    with jax.named_scope("sends"):
        for copy in pending:
            copy.wait_send()
        for k in range(CHUNKS):
            for by in range(SIDE):
                for c in range(CORES):
                    give(k, c, by, lambda copy: copy.wait_send())


def local(
    mix_in, mix_gain, w_in_x, w_in_y, conv_taps, recur_gate_w, input_gate_w, decay_logit, decay_shift,
    moe_in, moe_gain, routes, route_weight, expert_gate, expert_up, expert_down,
):
    hbm = pl.BlockSpec(memory_space=pltpu.HBM)
    vmem = pl.BlockSpec(memory_space=pltpu.VMEM)
    dma = pltpu.SemaphoreType.DMA
    out = jax.ShapeDtypeStruct((ROWS, LANE), BF16)
    v = pltpu.VMEM
    return pl.pallas_call(
        kernel,
        out_shape=(out, out),
        in_specs=[hbm] * 16,
        out_specs=(vmem, vmem),
        scratch_shapes=[
            v((ROWS, D), BF16), v((ROWS, D), BF16), v((D, 2 * LANE), BF16), v((ROWS, LANE), F32),
            v((D, 2 * LANE), BF16), v((D, SIDE * LANE), BF16),
            v((1, D), F32), v((4, LANE), F32), v((1, LANE, LANE), BF16), v((1, LANE, LANE), BF16), v((1, LANE), F32),
            v((1, D), F32), v((2, ROWS), jnp.int32), v((2, ROWS), F32),
            v((ROWS, SLOTS), BF16), v((ROWS, SLOTS), BF16), v((EP, CAP, LANE), BF16),
            v((SIDE, SIDE, SLOTS, LANE), BF16), v((SLOTS, LANE), BF16), v((SIDE, SIDE, SLOTS // SIDE, LANE), BF16),
            v((CHUNKS * CORES, SIDE, CAP, LANE), BF16), v((EP, CAP, LANE), BF16),
            v((ROWS, LANE), BF16), v((ROWS + 8, LANE), F32), v((ROWS, LANE), BF16),
            v((16, LANE), BF16), v((16, LANE), BF16), v((ROWS, LANE), F32), v((ROWS, LANE), F32),
            v((2, LANE), F32), v((EP, 2, LANE), F32),
            dma((16,)), dma((CHUNKS * 16,)), dma((CHUNKS * 16,)), dma((CHUNKS * 4,)), dma((CHUNKS * 4,)),
            dma((CHUNKS * 3,)), dma((CHUNKS * 3,)), dma((PIECES * 3,)), dma((PIECES * 3,)), dma((EP,)), dma((EP,)),
            dma((EP,)), dma((EP,)), dma((EP,)), dma((EP,)), dma((2,)),
        ],
        compiler_params=pltpu.CompilerParams(
            collective_id=0, has_side_effects=True, vmem_limit_bytes=67043328
        ),
        name="mixer_and_experts",
    )(
        mix_in, moe_in, w_in_x, w_in_y, decay_shift, expert_gate, expert_up, expert_down,
        mix_gain.reshape(1, D), conv_taps, recur_gate_w, input_gate_w, decay_logit.reshape(1, LANE),
        moe_gain.reshape(1, D), routes.T, route_weight.T,
    )


def solution(mesh):
    placed = (
        P("ep", None),
        P(),
        P(None, "tp"),
        P(None, "tp"),
        P(None, "tp"),
        P("tp", None, None),
        P("tp", None, None),
        P("tp"),
        P("ep", "tp"),
        P("ep", None),
        P(),
        P("ep", None),
        P("ep", None),
        P("ep", None, "tp"),
        P("ep", None, "tp"),
        P("ep", None, "tp"),
    )
    return jax.shard_map(
        local, mesh=mesh, in_specs=placed, out_specs=(P("ep", "tp"), P("ep", "tp")), check_vma=False
    )
```

```python
import functools

import jax
import jax.numpy as jnp
from jax import lax
from jax.experimental import pallas as pl
from jax.experimental.pallas import tpu as pltpu
from jax.sharding import PartitionSpec as P

MESH = pl.DeviceIdType.MESH
F32 = jnp.float32
BF16 = jnp.bfloat16
epsilon = 1e-06
lru_scale = 8.0

RING = 16
CORES = 2
EP = RING * CORES
SIDE = 4
ROWS = 256
D = 2048
LANE = 128
CAP = 32
SLOTS = EP * CAP
CHUNKS = 8
CH = SLOTS // CHUNKS
QROWS = CH // SIDE
PIECES = 8
WROWS = D // PIECES

XROWS = [64, 96, 96, 64, 64, 32, 64, 96]

NEAR = [0, -1, 2, 1, 8, -7, -6, 7, -4, 5, 6, -5, 3, -3, 4, -2]
PLACE = {off % RING: at for at, off in enumerate(NEAR)}

def place_of(at, c):
    n = at % SIDE
    return at // SIDE * 2 * SIDE + (c + n) % 2 * SIDE + n


ORDER = [
    "MA0", "W10", "W11", "W12", "Y10", "Y11", "X10", "X11", "W14", "Y20", "Y21", "W15", "X21", "X20", "W16", "Y30",
    "MB0", "MC0", "X31", "Y31", "W20", "X30", "X12", "X13", "Y40", "Y12", "Y13", "Y41", "X15", "Y15", "X14", "Y14",
    "X17", "X41", "X16", "X22", "X23", "Y16", "W21", "X40", "Y23", "Y22", "Y17", "X25", "Y25", "X24", "Y24", "W22",
    "X32", "UP1", "X27", "X26", "UP0", "Y32", "X33", "Y33", "MD0", "X34", "Y34", "X42", "Y42", "Y35", "X35", "X43",
    "X36", "Y43", "Y44", "UP2", "X44", "X45", "W17", "Y26", "X37", "Y45", "UP3", "X46", "UP4", "Y36", "Y27", "B10",
    "B12", "B11", "W23", "UP5", "X47", "Y37", "B13", "B20", "Y46", "B22", "B14", "B21", "Y47", "B15", "DN0", "B23",
    "DN2", "UP6", "B24", "DN1", "UP7", "B25", "DN3", "DN4", "B16", "DN5", "B17", "B26", "B27", "DN6", "DN7",
]
EARLY = [3]


def softplus(v):
    e = jnp.exp(-jnp.abs(v))
    series = e * (1.0 - e * (1.0 / 2 - e * (1.0 / 3 - e * (1.0 / 4 - e * (1.0 / 5 - e / 6)))))
    return jnp.maximum(v, 0.0) + jnp.where(e < 0.03, series, jnp.log(1.0 + e))


def one_minus_exp(v):
    series = 1.0 + v / 8
    for n in (7, 6, 5, 4, 3, 2):
        series = 1.0 + v / n * series
    return jnp.where(v > -0.25, -v * series, 1.0 - jnp.exp(v))


def kernel(
    mix_in, moe_in, w_x, w_y, shift, w_gate, w_up, w_down,
    mix_gain, conv_taps, recur_w, input_w, logit, moe_gain, routes, weight,
    mixer_out, moe_out,
    mix_v, moe_v, win_v, shift_v, gu_v, wd,
    mix_gain_v, conv_taps_v, recur_v, input_v, logit_v, moe_gain_v, routes_v, weight_v,
    c0, c1, sent, X, hown, H, res, ret, ybr, xb, xcv, halo_out, halo_in, sa, sb, carry_out, carry_in,
    load_sem, x_send, x_recv, b_send, b_recv, a_send, a_recv, w_send, w_recv,
    d_send, d_recv, r_send, r_recv, k_send, k_recv, h_sem,
):
    ep, tp = lax.axis_index("ep"), lax.axis_index("tp")
    z, core = ep // CORES, lax.rem(ep, CORES)
    y, x = tp // SIDE, lax.rem(tp, SIDE)

    def wrap(v, n):
        return lax.rem(v + 2 * n, n)

    east, west = wrap(x + 1, SIDE), wrap(x - 1, SIDE)
    north, south = wrap(y + 1, SIDE), wrap(y - 1, SIDE)
    across = wrap(x + 2, SIDE)
    plane = [(ep, y * SIDE + east), (ep, y * SIDE + west), (ep, north * SIDE + x), (ep, south * SIDE + x)]
    row = [plane[0], plane[1], (ep, y * SIDE + across)]

    def by_x(values, of):
        got = values[0]
        for n in range(1, SIDE):
            got = jnp.where(of == n, values[n], got)
        return got

    def offset(m, of):
        return by_x(NEAR[SIDE * m : SIDE * (m + 1)], of)

    def lanes(n):
        return pl.ds(pl.multiple_of(n * LANE, LANE), LANE)

    def peer(at, c):
        return wrap(z + NEAR[at], RING) * CORES + c

    loads = {}
    for n, (name, src, dst) in enumerate([
        ("routes", routes, routes_v), ("down", w_down.at[0], wd.at[:, lanes(x)]), ("moe_gain", moe_gain, moe_gain_v), ("moe", moe_in, moe_v),
        ("mix_gain", mix_gain, mix_gain_v), ("mix", mix_in, mix_v),
        ("w_x", w_x, win_v.at[:, :LANE]), ("w_y", w_y, win_v.at[:, LANE:]),
        ("taps", conv_taps, conv_taps_v), ("recur", recur_w, recur_v), ("input", input_w, input_v),
        ("logit", logit, logit_v), ("shift", shift, shift_v),
        ("gate", w_gate.at[0], gu_v.at[:, :LANE]), ("up", w_up.at[0], gu_v.at[:, LANE:]),
        ("weight", weight, weight_v),
    ]):
        loads[name] = pltpu.make_async_copy(src, dst, load_sem.at[n])
        loads[name].start()

    def loaded(*names):
        for name in names:
            loads[name].wait()

    barrier = pltpu.get_barrier_semaphore()

    def greet(where):
        pl.semaphore_signal(barrier, inc=1, device_id=where, device_id_type=MESH)

    far = sorted(range(1, RING), key=lambda at: -abs(NEAR[at]))
    for at in far:
        for c in range(CORES):
            greet((peer(at, c), tp))
    for m in sorted(range(RING // SIDE), key=lambda m: -max(map(abs, NEAR[SIDE * m : SIDE * (m + 1)]))):
        for by in range(1, SIDE):
            other = wrap(x + by, SIDE)
            for c in range(CORES):
                greet((wrap(z + offset(m, x), RING) * CORES + c, y * SIDE + other))
                greet((wrap(z - offset(m, other), RING) * CORES + c, y * SIDE + other))
    greet((peer(0, 1 - core), tp))
    for where in plane + row[2:]:
        greet(where)
    greeted = len(plane) + 1 + EP - 1 + 2 * RING // SIDE * (SIDE - 1) * CORES

    pending = []

    def launch(src, dst, ss, rs, where):
        copy = pltpu.make_async_remote_copy(
            src_ref=src, dst_ref=dst, send_sem=ss, recv_sem=rs, device_id=where, device_id_type=MESH
        )
        copy.start()
        pending.append(copy)
        return copy

    def normed(ref, gain, lanes):
        v = ref[...].astype(F32)
        scale = lax.rsqrt(jnp.sum(v * v, axis=1, keepdims=True) / D + epsilon)
        if lanes is not None:
            v = ref[:, lanes].astype(F32)
            return (v * scale * gain[:, lanes]).astype(BF16)
        return (v * scale * gain[...]).astype(BF16)

    def columns(ref):
        flat = ref[...].astype(F32)
        return jnp.transpose(jnp.concatenate([flat] * 4, axis=0))

    lane_e = lax.broadcasted_iota(jnp.int32, (ROWS, LANE), 1)
    loaded("routes")
    chosen = columns(routes_v).astype(jnp.int32)
    onehot = [jnp.where(chosen[:, k : k + 1] == lane_e, 1.0, 0.0).astype(BF16) for k in range(2)]
    before = jnp.where(
        lax.broadcasted_iota(jnp.int32, (ROWS, ROWS), 1) < lax.broadcasted_iota(jnp.int32, (ROWS, ROWS), 0), 1.0, 0.0
    ).astype(BF16)
    rank = [jnp.dot(before, hot, preferred_element_type=F32) for hot in onehot]
    rank[1] = rank[1] + jnp.sum(onehot[0].astype(F32), axis=0, keepdims=True)
    lane_1 = lax.broadcasted_iota(jnp.int32, (1, LANE), 1)
    off = (lane_1 // CORES - z + 2 * RING) % RING
    at = jnp.zeros((1, LANE), jnp.int32)
    for n in range(1, RING):
        at = jnp.where(off == NEAR[n] % RING, n, at)
    base = (CAP * place_of(at, lane_1 % CORES)).astype(F32)
    slot_lane = lax.broadcasted_iota(jnp.int32, (ROWS, SLOTS), 1)
    for ref, hot, r in zip((c0, c1), onehot, rank):
        slot = jnp.sum(hot.astype(F32) * (r + base), axis=1, keepdims=True).astype(jnp.int32)
        ref[...] = jnp.where(slot_lane == slot, 1.0, 0.0).astype(BF16)

    loaded("moe", "moe_gain")
    own_rows = normed(moe_v, moe_gain_v, lanes(tp))
    sent[...] = lax.dot_general(
        c0[...] + c1[...], own_rows, (((0,), (0,)), ((), ())), preferred_element_type=F32
    ).astype(BF16).reshape(EP, CAP, LANE)

    with jax.named_scope("barrier"):
        pl.semaphore_wait(barrier, greeted)
    loaded("down")
    ways = {}

    def weights(step, q):
        if step == 1:
            views = [(wd.at[pl.ds(q * WROWS, WROWS), lanes(x)], q)] * 2
        else:
            ways["W", 1, q, 0].wait_recv()
            ways["W", 1, q + PIECES // 2, 1].wait_recv()
            views = [
                (wd.at[pl.ds(q * WROWS, WROWS), lanes(west)], PIECES + q),
                (wd.at[pl.ds((q + PIECES // 2) * WROWS, WROWS), lanes(east)], PIECES + q),
            ]
        for n, (view, slot) in enumerate(views):
            ways["W", step, q, n] = launch(view, view, w_send.at[2 * slot + n], w_recv.at[2 * slot + n], row[n])

    for q in EARLY:
        weights(1, q)

    def block(buf, p):
        return buf.at[y, x, pl.ds(pl.multiple_of(p * CAP, CAP), CAP)]

    def dispatch(at, c):
        local = place_of(PLACE[-NEAR[at] % RING], c)
        place = place_of(at, core)
        where = wrap(z - NEAR[at], RING) * CORES + c
        launch(sent.at[local], block(X, place), d_send.at[local], d_recv.at[place], (where, tp))

    dispatch(0, 1 - core)
    for at in range(1, RING):
        for c in range(CORES):
            dispatch(at, c)
    mine = place_of(0, core)
    X[y, x, pl.ds(pl.multiple_of(mine * CAP, CAP), CAP), :] = sent[mine]

    def arrived(p, sem, ref):
        pltpu.make_async_remote_copy(
            src_ref=ref, dst_ref=ref, send_sem=sem.at[p], recv_sem=sem.at[p],
            device_id=(ep, tp), device_id_type=MESH,
        ).wait_recv()

    def await_dispatch(k):
        if ("in", k) in ways:
            return
        ways["in", k] = None
        for p in range(k * CH // CAP, (k + 1) * CH // CAP):
            if p % SIDE or k > 1:
                arrived(p, d_recv, block(X, p))
            else:

                @pl.when(mine != p)
                def _():
                    arrived(p, d_recv, block(X, p))

    def gather(part, step, k):
        lo, size = k * CH, XROWS[k]
        if part == "Y":
            lo, size = lo + size, CH - size
        if size == 0:
            return
        full, first, second = pl.ds(lo, size), pl.ds(lo, size // 2), pl.ds(lo + size // 2, size // 2)
        along_x = (part == "X") == (step < 3)
        if step == 1:
            await_dispatch(k)
            views = [X.at[y, x, full]] * 2
        elif step == 2 and along_x:
            views = [X.at[y, west, first], X.at[y, east, second]]
        elif step == 2:
            views = [X.at[south, x, first], X.at[north, x, second]]
        elif step == 3 and along_x:
            views = [X.at[:, x, full]] * 2
        elif step == 3:
            views = [X.at[y, :, full]] * 2
        elif along_x:
            views = [X.at[:, west, first], X.at[:, east, second]]
        else:
            views = [X.at[south, :, first], X.at[north, :, second]]
        if step == 3:
            for n in range(2):
                ways[part, 2, k, n].wait_recv()
        for n in range(2):
            if step == 2 or step == 4:
                ways[part, step - 1, k, n].wait_recv()
            slot = ((("XY".index(part) * CHUNKS) + k) * 4 + step - 1) * 2 + n
            ways[part, step, k, n] = launch(
                views[n], views[n], x_send.at[slot], x_recv.at[slot], plane[n if along_x else 2 + n]
            )

    def all_blocks(buf, rows):
        return jnp.concatenate([buf[a, b, rows, :] for a in range(SIDE) for b in range(SIDE)], axis=1)

    def quarter(k, n):
        return pl.ds(pl.multiple_of(k * CH + n * QROWS, QROWS), QROWS)

    def run_up(k):
        for part in "XY":
            for n in range(2):
                if (part, 4, k, n) in ways:
                    ways[part, 4, k, n].wait_recv()
        if "up" not in ways:
            ways["up"] = loaded("gate", "up")
        both = jnp.dot(all_blocks(X, pl.ds(k * CH, CH)), gu_v[...], preferred_element_type=F32)
        g, u = both[:, :LANE], both[:, LANE:]
        hown[pl.ds(k * CH, CH), :] = (g * jax.nn.sigmoid(g) * u).astype(BF16)
        ours = pl.ds(k * QROWS, QROWS)
        for n, who in enumerate((east, west, across)):
            slot = 3 * k + n
            ways["A", k, n] = launch(hown.at[quarter(k, who)], H.at[y, x, ours], a_send.at[slot], a_recv.at[slot], row[n])
        H[y, x, ours, :] = hown[quarter(k, x), :]

    def spread(step, k):
        slot = 4 * k + 2 * (step - 1)
        lo = k * QROWS
        if step == 1:
            for n, who in enumerate((west, east, across)):
                ways["A", k, n].wait_recv()
            views = [H.at[y, :, pl.ds(lo, QROWS)]] * 2
        else:
            views = [H.at[south, :, pl.ds(lo, QROWS // 2)], H.at[north, :, pl.ds(lo + QROWS // 2, QROWS // 2)]]
        for n in range(2):
            if step == 2:
                ways["B", 1, k, n].wait_recv()
            ways["B", step, k, n] = launch(views[n], views[n], b_send.at[slot + n], b_recv.at[slot + n], plane[2 + n])

    def give(k, by, act):
        other, m = wrap(x + by, SIDE), k // 2
        place = by_x([place_of(PLACE[-v % RING], core) for v in NEAR[SIDE * m : SIDE * (m + 1)]], x)
        slot = k * SIDE + by
        copy = pltpu.make_async_remote_copy(
            src_ref=res.at[k, other], dst_ref=ret.at[place], send_sem=r_send.at[slot], recv_sem=r_recv.at[place],
            device_id=(wrap(z + offset(m, x), RING) * CORES + (x + k) % CORES, y * SIDE + other), device_id_type=MESH,
        )
        if k < CORES and by == 0:
            stays = jnp.logical_and(x == 0, core == k)

            @pl.when(jnp.logical_not(stays))
            def _():
                act(copy)

            if act is starts:

                @pl.when(stays)
                def _():
                    ret[mine] = res[k, 0]

        else:
            act(copy)

    def starts(copy):
        copy.start()

    def run_down(k):
        for n in range(2):
            ways["B", 2, k, n].wait_recv()
        if "down" not in ways:
            ways["down"] = None
            for q in range(PIECES // 2):
                ways["W", 1, q, 1].wait_recv()
                ways["W", 1, q + PIECES // 2, 0].wait_recv()
                ways["W", 2, q, 0].wait_recv()
                ways["W", 2, q, 1].wait_recv()
        out = jnp.dot(all_blocks(H, pl.ds(k * QROWS, QROWS)), wd[...], preferred_element_type=F32).astype(BF16)
        for n in range(SIDE):
            res[k, n] = out[:, n * LANE : (n + 1) * LANE]
        for by in range(SIDE):
            give(k, by, starts)

    def mix_a():
        loaded("mix", "mix_gain", "w_x", "w_y")
        rows = normed(mix_v, mix_gain_v, None)
        both = jnp.dot(rows, win_v[...], preferred_element_type=F32).astype(BF16)
        ybr[...] = both[:, LANE:]
        xb[pl.ds(8, ROWS), :] = both[:, :LANE].astype(F32)
        halo_out[...] = both[ROWS - 16 :, :LANE]
        ways["halo"] = launch(halo_out, halo_in, h_sem.at[0], h_sem.at[1], (wrap(ep + 1, EP), tp))

    def mix_b():
        ways["halo"].wait_recv()
        loaded("taps", "recur", "input", "logit", "shift")
        xb[pl.ds(0, 8), :] = jnp.where(ep > 0, halo_in[...].astype(F32)[8:], 0.0)
        conv = jnp.zeros((ROWS, LANE), F32)
        for k in range(4):
            conv = conv + conv_taps_v[k : k + 1, :] * xb[pl.ds(5 + k, ROWS), :]
        x_conv = conv.astype(BF16)
        xcv[...] = x_conv
        gate_a = jnp.dot(x_conv, recur_v[0], preferred_element_type=F32)
        gate_x = jnp.dot(x_conv, input_v[0], preferred_element_type=F32)
        log_decay = -lru_scale * jax.nn.sigmoid(gate_a) * softplus(-logit_v[...]) + shift_v[...]
        sa[...] = jnp.exp(log_decay)
        sb[...] = jnp.sqrt(one_minus_exp(2.0 * log_decay)) * jax.nn.sigmoid(gate_x) * x_conv.astype(F32)

    def mix_c():
        a, b = sa[...], sb[...]
        row = lax.broadcasted_iota(jnp.int32, (ROWS, LANE), 0)
        by = 1
        while by < ROWS:
            behind = row >= by
            b = jnp.where(behind, a * pltpu.roll(b, by, 0), 0.0) + b
            a = jnp.where(behind, pltpu.roll(a, by, 0), 1.0) * a
            by *= 2
        sa[...] = a
        sb[...] = b
        carry_out[0:1, :] = a[ROWS - 1 :, :]
        carry_out[1:2, :] = b[ROWS - 1 :, :]

        def tell(at, c):
            where = peer(at, c)
            launch(carry_out, carry_in.at[ep], k_send.at[CORES * at + c], k_recv.at[ep], (where, tp))

        tell(0, 1 - core)
        for at in range(1, RING):
            for c in range(CORES):
                tell(at, c)
        carry_in[ep] = carry_out[...]

    def mix_d():
        for at in range(RING):
            for c in range(CORES):
                if at > 0 or c == 0:
                    who = peer(at, c) if at else peer(0, 1 - core)
                    arrived(who, k_recv, carry_in.at[who])
        state = jnp.zeros((1, LANE), F32)
        for e in range(EP):
            pair = carry_in[e]
            state = jnp.where(e < ep, pair[0:1] * state + pair[1:2], state)
        lru = sb[...] + sa[...] * state
        mixer_out[...] = (lru * jax.nn.gelu(ybr[...].astype(F32), approximate=True)).astype(BF16)

    for item in ORDER:
        what, k = item[:2], int(item[2:])
        with jax.named_scope(f"{what}_{k}"):
            if what == "UP":
                run_up(k)
            elif what == "DN":
                run_down(k)
            elif what[0] == "M":
                {"A": mix_a, "B": mix_b, "C": mix_c, "D": mix_d}[what[1]]()
            elif what[0] == "W":
                weights(int(what[1]), k)
            elif what[0] == "B":
                spread(int(what[1]), k)
            else:
                gather(what[0], int(what[1]), k)

    with jax.named_scope("sends"):
        for copy in pending:
            copy.wait_send()
        for k in range(CHUNKS):
            for by in range(SIDE):
                give(k, by, lambda copy: copy.wait_send())
    loaded("weight")
    w = columns(weight_v)
    total = w[:, 0:1] + w[:, 1:2]
    picked = [jnp.zeros((ROWS, LANE), F32)] * 2
    for half in range(2):
        blocks = range(half * EP // 2, (half + 1) * EP // 2)
        with jax.named_scope(f"back_{half}"):
            for p in blocks:
                if p not in (0, SIDE):
                    arrived(p, r_recv, ret.at[p])
            if half == 0:
                arrived(SIDE - mine, r_recv, ret.at[SIDE - mine])

                @pl.when(x != 0)
                def _():
                    arrived(mine, r_recv, ret.at[mine])

        part = pl.ds(half * SLOTS // 2, SLOTS // 2)
        back = ret[pl.ds(half * EP // 2, EP // 2)].reshape(SLOTS // 2, LANE)
        for n, ref in enumerate((c0, c1)):
            picked[n] = picked[n] + jnp.dot(ref[:, part], back, preferred_element_type=F32)
    moe_out[...] = (w[:, 0:1] / total * picked[0] + w[:, 1:2] / total * picked[1]).astype(BF16)


def local(
    mix_in, mix_gain, w_in_x, w_in_y, conv_taps, recur_gate_w, input_gate_w, decay_logit, decay_shift,
    moe_in, moe_gain, routes, route_weight, expert_gate, expert_up, expert_down,
):
    hbm = pl.BlockSpec(memory_space=pltpu.HBM)
    vmem = pl.BlockSpec(memory_space=pltpu.VMEM)
    dma = pltpu.SemaphoreType.DMA
    out = jax.ShapeDtypeStruct((ROWS, LANE), BF16)
    v = pltpu.VMEM
    return pl.pallas_call(
        kernel,
        out_shape=(out, out),
        in_specs=[hbm] * 16,
        out_specs=(vmem, vmem),
        scratch_shapes=[
            v((ROWS, D), BF16), v((ROWS, D), BF16), v((D, 2 * LANE), BF16), v((ROWS, LANE), F32),
            v((D, 2 * LANE), BF16), v((D, SIDE * LANE), BF16),
            v((1, D), F32), v((4, LANE), F32), v((1, LANE, LANE), BF16), v((1, LANE, LANE), BF16), v((1, LANE), F32),
            v((1, D), F32), v((2, ROWS), jnp.int32), v((2, ROWS), F32),
            v((ROWS, SLOTS), BF16), v((ROWS, SLOTS), BF16), v((EP, CAP, LANE), BF16),
            v((SIDE, SIDE, SLOTS, LANE), BF16), v((SLOTS, LANE), BF16), v((SIDE, SIDE, SLOTS // SIDE, LANE), BF16),
            v((CHUNKS, SIDE, CAP, LANE), BF16), v((EP, CAP, LANE), BF16),
            v((ROWS, LANE), BF16), v((ROWS + 8, LANE), F32), v((ROWS, LANE), BF16),
            v((16, LANE), BF16), v((16, LANE), BF16), v((ROWS, LANE), F32), v((ROWS, LANE), F32),
            v((2, LANE), F32), v((EP, 2, LANE), F32),
            dma((16,)), dma((CHUNKS * 16,)), dma((CHUNKS * 16,)), dma((CHUNKS * 4,)), dma((CHUNKS * 4,)),
            dma((CHUNKS * 3,)), dma((CHUNKS * 3,)), dma((PIECES * 3,)), dma((PIECES * 3,)), dma((EP,)), dma((EP,)),
            dma((EP,)), dma((EP,)), dma((EP,)), dma((EP,)), dma((2,)),
        ],
        compiler_params=pltpu.CompilerParams(
            collective_id=0, has_side_effects=True, vmem_limit_bytes=67043328
        ),
        name="mixer_and_experts",
    )(
        mix_in, moe_in, w_in_x, w_in_y, decay_shift, expert_gate, expert_up, expert_down,
        mix_gain.reshape(1, D), conv_taps, recur_gate_w, input_gate_w, decay_logit.reshape(1, LANE),
        moe_gain.reshape(1, D), routes.T, route_weight.T,
    )


def solution(mesh):
    placed = (
        P("ep", None),
        P(),
        P(None, "tp"),
        P(None, "tp"),
        P(None, "tp"),
        P("tp", None, None),
        P("tp", None, None),
        P("tp"),
        P("ep", "tp"),
        P("ep", None),
        P(),
        P("ep", None),
        P("ep", None),
        P("ep", None, "tp"),
        P("ep", None, "tp"),
        P("ep", None, "tp"),
    )
    return jax.shard_map(
        local, mesh=mesh, in_specs=placed, out_specs=(P("ep", "tp"), P("ep", "tp")), check_vma=False
    )
```

```python
import functools

import jax
import jax.numpy as jnp
from jax import lax
from jax.experimental import pallas as pl
from jax.experimental.pallas import tpu as pltpu
from jax.sharding import PartitionSpec as P

MESH = pl.DeviceIdType.MESH
F32 = jnp.float32
BF16 = jnp.bfloat16
epsilon = 1e-06
lru_scale = 8.0

RING = 16
CORES = 2
EP = RING * CORES
SIDE = 4
ROWS = 256
D = 2048
LANE = 128
CAP = 32
SLOTS = EP * CAP
CHUNKS = 8
CH = SLOTS // CHUNKS
QROWS = CH // SIDE
PIECES = 8
WROWS = D // PIECES

XROWS = [128, 128, 64, 64, 64, 64, 64, 64]

NEAR = [0, -1, 2, 1, 8, -7, -6, 7, -4, 5, 6, -5, 3, -3, 4, -2]
PLACE = {off % RING: at for at, off in enumerate(NEAR)}

def place_of(at, c):
    n = at % SIDE
    return at // SIDE * 2 * SIDE + (c + n) % 2 * SIDE + n


STRAIGHT = []

FINE = [0, 1]

ORDER = [
    "MA0", "W11", "W12", "W13", "Xa0", "Xa1", "X11", "X10", "W15", "Xd0", "W16", "Xd1", "Xb1", "X21", "X20", "Xb0",
    "W17", "MB0", "W21", "MC0", "Xc1", "W22", "Xc0", "Xe1", "Y12", "X12", "X13", "Xe0", "W23", "Y13", "Xf1", "Y14",
    "X14", "Y15", "X15", "Xf0", "X16", "Y17", "X17", "Y16", "X22", "Y22", "X23", "W14", "Y23", "UP1", "Y24", "X24",
    "Y25", "X25", "UP0", "X26", "Y27", "X27", "X32", "Y32", "Y26", "X33", "Y33", "MD0", "X34", "Y34", "B10", "Y35",
    "B11", "X42", "Y42", "X43", "Y43", "X35", "Y36", "B20", "Y44", "X44", "Y45", "B21", "X36", "UP2", "Y37", "UP3",
    "X37", "Y46", "X45", "UP4", "W20", "B12", "X46", "Y47", "X47", "B13", "UP5", "B14", "B22", "DN0", "DN1", "UP6",
    "UP7", "B23", "B24", "B15", "DN2", "B16", "DN3", "B17", "DN4", "B25", "B26", "B27", "DN5", "DN6", "DN7",
]
EARLY = [0]


def softplus(v):
    e = jnp.exp(-jnp.abs(v))
    series = e * (1.0 - e * (1.0 / 2 - e * (1.0 / 3 - e * (1.0 / 4 - e * (1.0 / 5 - e / 6)))))
    return jnp.maximum(v, 0.0) + jnp.where(e < 0.03, series, jnp.log(1.0 + e))


def one_minus_exp(v):
    series = 1.0 + v / 8
    for n in (7, 6, 5, 4, 3, 2):
        series = 1.0 + v / n * series
    return jnp.where(v > -0.25, -v * series, 1.0 - jnp.exp(v))


def kernel(
    mix_in, moe_in, w_x, w_y, shift, w_gate, w_up, w_down,
    mix_gain, conv_taps, recur_w, input_w, logit, moe_gain, routes, weight,
    mixer_out, moe_out,
    mix_v, moe_v, win_v, shift_v, gu_v, wd,
    mix_gain_v, conv_taps_v, recur_v, input_v, logit_v, moe_gain_v, routes_v, weight_v,
    c0, c1, sent, X, hown, H, res, ret, ybr, xb, xcv, halo_out, halo_in, sa, sb, carry_out, carry_in,
    load_sem, x_send, x_recv, b_send, b_recv, a_send, a_recv, w_send, w_recv, f_send, f_recv,
    d_send, d_recv, r_send, r_recv, k_send, k_recv, h_sem,
):
    ep, tp = lax.axis_index("ep"), lax.axis_index("tp")
    z, core = ep // CORES, lax.rem(ep, CORES)
    y, x = tp // SIDE, lax.rem(tp, SIDE)

    def wrap(v, n):
        return lax.rem(v + 2 * n, n)

    east, west = wrap(x + 1, SIDE), wrap(x - 1, SIDE)
    north, south = wrap(y + 1, SIDE), wrap(y - 1, SIDE)
    across = wrap(x + 2, SIDE)
    plane = [(ep, y * SIDE + east), (ep, y * SIDE + west), (ep, north * SIDE + x), (ep, south * SIDE + x)]
    row = [plane[0], plane[1], (ep, y * SIDE + across)]
    others = [(dx, wrap(y + dy, SIDE)) for dy in range(SIDE) for dx in range(SIDE) if dx or dy]

    def by_x(values, of):
        got = values[0]
        for n in range(1, SIDE):
            got = jnp.where(of == n, values[n], got)
        return got

    def offset(m, of):
        return by_x(NEAR[SIDE * m : SIDE * (m + 1)], of)

    def lanes(n):
        return pl.ds(pl.multiple_of(n * LANE, LANE), LANE)

    def peer(at, c):
        return wrap(z + NEAR[at], RING) * CORES + c

    loads = {}
    for n, (name, src, dst) in enumerate([
        ("routes", routes, routes_v), ("down", w_down.at[0], wd.at[:, lanes(x)]), ("moe_gain", moe_gain, moe_gain_v), ("moe", moe_in, moe_v),
        ("mix_gain", mix_gain, mix_gain_v), ("mix", mix_in, mix_v),
        ("w_x", w_x, win_v.at[:, :LANE]), ("w_y", w_y, win_v.at[:, LANE:]),
        ("taps", conv_taps, conv_taps_v), ("recur", recur_w, recur_v), ("input", input_w, input_v),
        ("logit", logit, logit_v), ("shift", shift, shift_v),
        ("gate", w_gate.at[0], gu_v.at[:, :LANE]), ("up", w_up.at[0], gu_v.at[:, LANE:]),
        ("weight", weight, weight_v),
    ]):
        loads[name] = pltpu.make_async_copy(src, dst, load_sem.at[n])
        loads[name].start()

    def loaded(*names):
        for name in names:
            loads[name].wait()

    barrier = pltpu.get_barrier_semaphore()

    def greet(where):
        pl.semaphore_signal(barrier, inc=1, device_id=where, device_id_type=MESH)

    far = sorted(range(1, RING), key=lambda at: -abs(NEAR[at]))
    for at in far:
        for c in range(CORES):
            greet((peer(at, c), tp))
    for m in sorted(range(RING // SIDE), key=lambda m: -max(map(abs, NEAR[SIDE * m : SIDE * (m + 1)]))):
        for by in range(1, SIDE):
            other = wrap(x + by, SIDE)
            for c in range(CORES):
                greet((wrap(z + offset(m, x), RING) * CORES + c, y * SIDE + other))
                greet((wrap(z - offset(m, other), RING) * CORES + c, y * SIDE + other))
    greet((peer(0, 1 - core), tp))
    for dx, its_y in others:
        greet((ep, its_y * SIDE + wrap(x + dx, SIDE)))
    greeted = len(others) + EP - 1 + 2 * RING // SIDE * (SIDE - 1) * CORES

    pending = []

    def launch(src, dst, ss, rs, where):
        copy = pltpu.make_async_remote_copy(
            src_ref=src, dst_ref=dst, send_sem=ss, recv_sem=rs, device_id=where, device_id_type=MESH
        )
        copy.start()
        pending.append(copy)
        return copy

    def normed(ref, gain, lanes):
        v = ref[...].astype(F32)
        scale = lax.rsqrt(jnp.sum(v * v, axis=1, keepdims=True) / D + epsilon)
        if lanes is not None:
            v = ref[:, lanes].astype(F32)
            return (v * scale * gain[:, lanes]).astype(BF16)
        return (v * scale * gain[...]).astype(BF16)

    def columns(ref):
        flat = ref[...].astype(F32)
        return jnp.transpose(jnp.concatenate([flat] * 4, axis=0))

    lane_e = lax.broadcasted_iota(jnp.int32, (ROWS, LANE), 1)
    loaded("routes")
    chosen = columns(routes_v).astype(jnp.int32)
    onehot = [jnp.where(chosen[:, k : k + 1] == lane_e, 1.0, 0.0).astype(BF16) for k in range(2)]
    before = jnp.where(
        lax.broadcasted_iota(jnp.int32, (ROWS, ROWS), 1) < lax.broadcasted_iota(jnp.int32, (ROWS, ROWS), 0), 1.0, 0.0
    ).astype(BF16)
    rank = [jnp.dot(before, hot, preferred_element_type=F32) for hot in onehot]
    rank[1] = rank[1] + jnp.sum(onehot[0].astype(F32), axis=0, keepdims=True)
    lane_1 = lax.broadcasted_iota(jnp.int32, (1, LANE), 1)
    off = (lane_1 // CORES - z + 2 * RING) % RING
    at = jnp.zeros((1, LANE), jnp.int32)
    for n in range(1, RING):
        at = jnp.where(off == NEAR[n] % RING, n, at)
    base = (CAP * place_of(at, lane_1 % CORES)).astype(F32)
    slot_lane = lax.broadcasted_iota(jnp.int32, (ROWS, SLOTS), 1)
    for ref, hot, r in zip((c0, c1), onehot, rank):
        slot = jnp.sum(hot.astype(F32) * (r + base), axis=1, keepdims=True).astype(jnp.int32)
        ref[...] = jnp.where(slot_lane == slot, 1.0, 0.0).astype(BF16)

    loaded("moe", "moe_gain")
    own_rows = normed(moe_v, moe_gain_v, lanes(tp))
    sent[...] = lax.dot_general(
        c0[...] + c1[...], own_rows, (((0,), (0,)), ((), ())), preferred_element_type=F32
    ).astype(BF16).reshape(EP, CAP, LANE)

    with jax.named_scope("barrier"):
        pl.semaphore_wait(barrier, greeted)
    loaded("down")
    ways, got = {}, set()

    def received(*key):
        if key not in got:
            got.add(key)
            ways[key].wait_recv()

    def weights(step, q):
        if step == 1:
            views = [(wd.at[pl.ds(q * WROWS, WROWS), lanes(x)], q)] * 2
        else:
            received("W", 1, q, 0)
            received("W", 1, q + PIECES // 2, 1)
            views = [
                (wd.at[pl.ds(q * WROWS, WROWS), lanes(west)], PIECES + q),
                (wd.at[pl.ds((q + PIECES // 2) * WROWS, WROWS), lanes(east)], PIECES + q),
            ]
        for n, (view, slot) in enumerate(views):
            ways["W", step, q, n] = launch(view, view, w_send.at[2 * slot + n], w_recv.at[2 * slot + n], row[n])

    for q in EARLY:
        weights(1, q)

    def block(buf, p):
        return buf.at[y, x, pl.ds(pl.multiple_of(p * CAP, CAP), CAP)]

    def dispatch(at, c):
        local = place_of(PLACE[-NEAR[at] % RING], c)
        place = place_of(at, core)
        where = wrap(z - NEAR[at], RING) * CORES + c
        launch(sent.at[local], block(X, place), d_send.at[local], d_recv.at[place], (where, tp))

    dispatch(0, 1 - core)
    for at in range(1, RING):
        for c in range(CORES):
            dispatch(at, c)
    mine = place_of(0, core)
    X[y, x, pl.ds(pl.multiple_of(mine * CAP, CAP), CAP), :] = sent[mine]

    def arrived(p, sem, ref):
        pltpu.make_async_remote_copy(
            src_ref=ref, dst_ref=ref, send_sem=sem.at[p], recv_sem=sem.at[p],
            device_id=(ep, tp), device_id_type=MESH,
        ).wait_recv()

    def await_dispatch(k):
        if ("in", k) in ways:
            return
        ways["in", k] = None
        for p in range(k * CH // CAP, (k + 1) * CH // CAP):
            if p % SIDE or k > 1:
                arrived(p, d_recv, block(X, p))
            else:

                @pl.when(mine != p)
                def _():
                    arrived(p, d_recv, block(X, p))

    def gather(part, step, k):
        lo, size = k * CH, XROWS[k]
        if part == "Y":
            lo, size = lo + size, CH - size
        if size == 0:
            return
        full, first, second = pl.ds(lo, size), pl.ds(lo, size // 2), pl.ds(lo + size // 2, size // 2)
        along_x = (part == "X") == (step < 3)
        if step == 1:
            await_dispatch(k)
            views = [X.at[y, x, full]] * 2
        elif step == 2 and along_x:
            views = [X.at[y, west, first], X.at[y, east, second]]
        elif step == 2:
            views = [X.at[south, x, first], X.at[north, x, second]]
        elif step == 3 and along_x:
            views = [X.at[:, x, full]] * 2
        elif step == 3:
            views = [X.at[y, :, full]] * 2
        elif along_x:
            views = [X.at[:, west, first], X.at[:, east, second]]
        else:
            views = [X.at[south, :, first], X.at[north, :, second]]
        if step == 3:
            for n in range(2):
                received(part, 2, k, n)
        for n in range(2):
            if step == 2 or step == 4:
                received(part, step - 1, k, n)
            slot = ((("XY".index(part) * CHUNKS) + k) * 4 + step - 1) * 2 + n
            ways[part, step, k, n] = launch(
                views[n], views[n], x_send.at[slot], x_recv.at[slot], plane[n if along_x else 2 + n]
            )

    def fine(letter, k):
        lo = k * CH
        full, first, second = pl.ds(lo, CH), pl.ds(lo, CH // 2), pl.ds(lo + CH // 2, CH // 2)
        stage, at = divmod("abcdef".index(letter), 3)
        cols = ([x], [west, east], [across])[at]
        if letter == "a":
            await_dispatch(k)
        for step in range(1, at + 1 if stage == 0 else 1):
            for n in range(2):
                received("X", step, k, n)
        for i, col in enumerate(cols):
            for n in range(2):
                if stage == 0:
                    view = X.at[y, col, full]
                else:
                    received("F", "abc"[at], k, i, n)
                    view = X.at[south, col, first] if n == 0 else X.at[north, col, second]
                slot = (FINE.index(k) * 6 + "abcdef".index(letter)) * 4 + 2 * i + n
                ways["F", letter, k, i, n] = launch(view, view, f_send.at[slot], f_recv.at[slot], plane[2 + n])

    def all_blocks(buf, rows):
        return jnp.concatenate([buf[a, b, rows, :] for a in range(SIDE) for b in range(SIDE)], axis=1)

    def quarter(k, n):
        return pl.ds(pl.multiple_of(k * CH + n * QROWS, QROWS), QROWS)

    def run_up(k):
        for part in "XY":
            for n in range(2):
                if (part, 4, k, n) in ways:
                    received(part, 4, k, n)
        for key in [key for key in ways if key[0] == "F" and key[1] in "def" and key[2] == k]:
            received(*key)
        if "up" not in ways:
            ways["up"] = loaded("gate", "up")
        both = jnp.dot(all_blocks(X, pl.ds(k * CH, CH)), gu_v[...], preferred_element_type=F32)
        g, u = both[:, :LANE], both[:, LANE:]
        hown[pl.ds(k * CH, CH), :] = (g * jax.nn.sigmoid(g) * u).astype(BF16)
        ours = pl.ds(k * QROWS, QROWS)
        if k in STRAIGHT:
            for n, (dx, its_y) in enumerate(others):
                slot = 3 * CHUNKS + STRAIGHT.index(k) * len(others) + n
                who = wrap(x + dx, SIDE)
                ways["S", k, n] = launch(
                    hown.at[quarter(k, who)], H.at[y, x, ours], a_send.at[slot], a_recv.at[slot], (ep, its_y * SIDE + who)
                )
        for n, who in enumerate(() if k in STRAIGHT else (east, west, across)):
            slot = 3 * k + n
            ways["A", k, n] = launch(hown.at[quarter(k, who)], H.at[y, x, ours], a_send.at[slot], a_recv.at[slot], row[n])
        H[y, x, ours, :] = hown[quarter(k, x), :]

    def spread(step, k):
        slot = 4 * k + 2 * (step - 1)
        lo = k * QROWS
        if step == 1:
            for n, who in enumerate((west, east, across)):
                received("A", k, n)
            views = [H.at[y, :, pl.ds(lo, QROWS)]] * 2
        else:
            views = [H.at[south, :, pl.ds(lo, QROWS // 2)], H.at[north, :, pl.ds(lo + QROWS // 2, QROWS // 2)]]
        for n in range(2):
            if step == 2:
                received("B", 1, k, n)
            ways["B", step, k, n] = launch(views[n], views[n], b_send.at[slot + n], b_recv.at[slot + n], plane[2 + n])

    def give(k, by, act):
        other, m = wrap(x + by, SIDE), k // 2
        place = by_x([place_of(PLACE[-v % RING], core) for v in NEAR[SIDE * m : SIDE * (m + 1)]], x)
        slot = k * SIDE + by
        copy = pltpu.make_async_remote_copy(
            src_ref=res.at[k, other], dst_ref=ret.at[place], send_sem=r_send.at[slot], recv_sem=r_recv.at[place],
            device_id=(wrap(z + offset(m, x), RING) * CORES + (x + k) % CORES, y * SIDE + other), device_id_type=MESH,
        )
        if k < CORES and by == 0:
            stays = jnp.logical_and(x == 0, core == k)

            @pl.when(jnp.logical_not(stays))
            def _():
                act(copy)

            if act is starts:

                @pl.when(stays)
                def _():
                    ret[mine] = res[k, 0]

        else:
            act(copy)

    def starts(copy):
        copy.start()

    def run_down(k):
        if k in STRAIGHT:
            for n in range(len(others)):
                received("S", k, n)
        for n in range(0 if k in STRAIGHT else 2):
            received("B", 2, k, n)
        if "down" not in ways:
            ways["down"] = None
            for q in range(PIECES // 2):
                received("W", 1, q, 1)
                received("W", 1, q + PIECES // 2, 0)
                received("W", 2, q, 0)
                received("W", 2, q, 1)
        out = jnp.dot(all_blocks(H, pl.ds(k * QROWS, QROWS)), wd[...], preferred_element_type=F32).astype(BF16)
        for n in range(SIDE):
            res[k, n] = out[:, n * LANE : (n + 1) * LANE]
        for by in range(SIDE):
            give(k, by, starts)

    def mix_a():
        loaded("mix", "mix_gain", "w_x", "w_y")
        rows = normed(mix_v, mix_gain_v, None)
        both = jnp.dot(rows, win_v[...], preferred_element_type=F32).astype(BF16)
        ybr[...] = both[:, LANE:]
        xb[pl.ds(8, ROWS), :] = both[:, :LANE].astype(F32)
        halo_out[...] = both[ROWS - 16 :, :LANE]
        ways["halo",] = launch(halo_out, halo_in, h_sem.at[0], h_sem.at[1], (wrap(ep + 1, EP), tp))

    def mix_b():
        received("halo")
        loaded("taps", "recur", "input", "logit", "shift")
        xb[pl.ds(0, 8), :] = jnp.where(ep > 0, halo_in[...].astype(F32)[8:], 0.0)
        conv = jnp.zeros((ROWS, LANE), F32)
        for k in range(4):
            conv = conv + conv_taps_v[k : k + 1, :] * xb[pl.ds(5 + k, ROWS), :]
        x_conv = conv.astype(BF16)
        xcv[...] = x_conv
        gate_a = jnp.dot(x_conv, recur_v[0], preferred_element_type=F32)
        gate_x = jnp.dot(x_conv, input_v[0], preferred_element_type=F32)
        log_decay = -lru_scale * jax.nn.sigmoid(gate_a) * softplus(-logit_v[...]) + shift_v[...]
        sa[...] = jnp.exp(log_decay)
        sb[...] = jnp.sqrt(one_minus_exp(2.0 * log_decay)) * jax.nn.sigmoid(gate_x) * x_conv.astype(F32)

    def mix_c():
        a, b = sa[...], sb[...]
        row = lax.broadcasted_iota(jnp.int32, (ROWS, LANE), 0)
        by = 1
        while by < ROWS:
            behind = row >= by
            b = jnp.where(behind, a * pltpu.roll(b, by, 0), 0.0) + b
            a = jnp.where(behind, pltpu.roll(a, by, 0), 1.0) * a
            by *= 2
        sa[...] = a
        sb[...] = b
        carry_out[0:1, :] = a[ROWS - 1 :, :]
        carry_out[1:2, :] = b[ROWS - 1 :, :]

        def tell(at, c):
            where = peer(at, c)
            launch(carry_out, carry_in.at[ep], k_send.at[CORES * at + c], k_recv.at[ep], (where, tp))

        tell(0, 1 - core)
        for at in range(1, RING):
            for c in range(CORES):
                tell(at, c)
        carry_in[ep] = carry_out[...]

    def mix_d():
        for at in range(RING):
            for c in range(CORES):
                if at > 0 or c == 0:
                    who = peer(at, c) if at else peer(0, 1 - core)
                    arrived(who, k_recv, carry_in.at[who])
        state = jnp.zeros((1, LANE), F32)
        for e in range(EP):
            pair = carry_in[e]
            state = jnp.where(e < ep, pair[0:1] * state + pair[1:2], state)
        lru = sb[...] + sa[...] * state
        mixer_out[...] = (lru * jax.nn.gelu(ybr[...].astype(F32), approximate=True)).astype(BF16)

    for item in ORDER:
        what, k = item[:2], int(item[2:])
        with jax.named_scope(f"{what}_{k}"):
            if what == "UP":
                run_up(k)
            elif what == "DN":
                run_down(k)
            elif what[0] == "M":
                {"A": mix_a, "B": mix_b, "C": mix_c, "D": mix_d}[what[1]]()
            elif what[0] == "W":
                weights(int(what[1]), k)
            elif what[0] == "B":
                spread(int(what[1]), k)
            elif what[1] in "abcdef":
                fine(what[1], k)
            else:
                gather(what[0], int(what[1]), k)

    with jax.named_scope("sends"):
        for copy in pending:
            copy.wait_send()
        for k in range(CHUNKS):
            for by in range(SIDE):
                give(k, by, lambda copy: copy.wait_send())
    loaded("weight")
    w = columns(weight_v)
    total = w[:, 0:1] + w[:, 1:2]
    picked = [jnp.zeros((ROWS, LANE), F32)] * 2
    for half in range(2):
        blocks = range(half * EP // 2, (half + 1) * EP // 2)
        with jax.named_scope(f"back_{half}"):
            for p in blocks:
                if p not in (0, SIDE):
                    arrived(p, r_recv, ret.at[p])
            if half == 0:
                arrived(SIDE - mine, r_recv, ret.at[SIDE - mine])

                @pl.when(x != 0)
                def _():
                    arrived(mine, r_recv, ret.at[mine])

        part = pl.ds(half * SLOTS // 2, SLOTS // 2)
        back = ret[pl.ds(half * EP // 2, EP // 2)].reshape(SLOTS // 2, LANE)
        for n, ref in enumerate((c0, c1)):
            picked[n] = picked[n] + jnp.dot(ref[:, part], back, preferred_element_type=F32)
    moe_out[...] = (w[:, 0:1] / total * picked[0] + w[:, 1:2] / total * picked[1]).astype(BF16)


def local(
    mix_in, mix_gain, w_in_x, w_in_y, conv_taps, recur_gate_w, input_gate_w, decay_logit, decay_shift,
    moe_in, moe_gain, routes, route_weight, expert_gate, expert_up, expert_down,
):
    hbm = pl.BlockSpec(memory_space=pltpu.HBM)
    vmem = pl.BlockSpec(memory_space=pltpu.VMEM)
    dma = pltpu.SemaphoreType.DMA
    out = jax.ShapeDtypeStruct((ROWS, LANE), BF16)
    v = pltpu.VMEM
    fines = 24 * len(FINE)
    straight = CHUNKS * 3 + len(STRAIGHT) * (SIDE * SIDE - 1)
    return pl.pallas_call(
        kernel,
        out_shape=(out, out),
        in_specs=[hbm] * 16,
        out_specs=(vmem, vmem),
        scratch_shapes=[
            v((ROWS, D), BF16), v((ROWS, D), BF16), v((D, 2 * LANE), BF16), v((ROWS, LANE), F32),
            v((D, 2 * LANE), BF16), v((D, SIDE * LANE), BF16),
            v((1, D), F32), v((4, LANE), F32), v((1, LANE, LANE), BF16), v((1, LANE, LANE), BF16), v((1, LANE), F32),
            v((1, D), F32), v((2, ROWS), jnp.int32), v((2, ROWS), F32),
            v((ROWS, SLOTS), BF16), v((ROWS, SLOTS), BF16), v((EP, CAP, LANE), BF16),
            v((SIDE, SIDE, SLOTS, LANE), BF16), v((SLOTS, LANE), BF16), v((SIDE, SIDE, SLOTS // SIDE, LANE), BF16),
            v((CHUNKS, SIDE, CAP, LANE), BF16), v((EP, CAP, LANE), BF16),
            v((ROWS, LANE), BF16), v((ROWS + 8, LANE), F32), v((ROWS, LANE), BF16),
            v((16, LANE), BF16), v((16, LANE), BF16), v((ROWS, LANE), F32), v((ROWS, LANE), F32),
            v((2, LANE), F32), v((EP, 2, LANE), F32),
            dma((16,)), dma((CHUNKS * 16,)), dma((CHUNKS * 16,)), dma((CHUNKS * 4,)), dma((CHUNKS * 4,)),
            dma((straight,)), dma((straight,)), dma((PIECES * 3,)), dma((PIECES * 3,)), dma((fines,)), dma((fines,)), dma((EP,)), dma((EP,)),
            dma((EP,)), dma((EP,)), dma((EP,)), dma((EP,)), dma((2,)),
        ],
        compiler_params=pltpu.CompilerParams(
            collective_id=0, has_side_effects=True, vmem_limit_bytes=67043328
        ),
        name="mixer_and_experts",
    )(
        mix_in, moe_in, w_in_x, w_in_y, decay_shift, expert_gate, expert_up, expert_down,
        mix_gain.reshape(1, D), conv_taps, recur_gate_w, input_gate_w, decay_logit.reshape(1, LANE),
        moe_gain.reshape(1, D), routes.T, route_weight.T,
    )


def solution(mesh):
    placed = (
        P("ep", None),
        P(),
        P(None, "tp"),
        P(None, "tp"),
        P(None, "tp"),
        P("tp", None, None),
        P("tp", None, None),
        P("tp"),
        P("ep", "tp"),
        P("ep", None),
        P(),
        P("ep", None),
        P("ep", None),
        P("ep", None, "tp"),
        P("ep", None, "tp"),
        P("ep", None, "tp"),
    )
    return jax.shard_map(
        local, mesh=mesh, in_specs=placed, out_specs=(P("ep", "tp"), P("ep", "tp")), check_vma=False
    )
```

```python
import functools

import jax
import jax.numpy as jnp
from jax import lax
from jax.experimental import pallas as pl
from jax.experimental.pallas import tpu as pltpu
from jax.sharding import PartitionSpec as P

MESH = pl.DeviceIdType.MESH
F32 = jnp.float32
BF16 = jnp.bfloat16
epsilon = 1e-06
lru_scale = 8.0

RING = 16
CORES = 2
EP = RING * CORES
SIDE = 4
ROWS = 256
D = 2048
LANE = 128
CAP = 32
SLOTS = EP * CAP
CHUNKS = 8
CH = SLOTS // CHUNKS
QROWS = CH // SIDE
PIECES = 8
WROWS = D // PIECES

XROWS = [128, 128, 64, 64, 64, 64, 64, 64]

NEAR = [0, -1, 2, 1, 8, -7, -6, 7, -4, 5, 6, -5, 3, -3, 4, -2]
PLACE = {off % RING: at for at, off in enumerate(NEAR)}

def place_of(at, c):
    n = at % SIDE
    return at // SIDE * 2 * SIDE + (c + n) % 2 * SIDE + n


STRAIGHT = []

FINE = [0, 1]

ORDER = [
    "MA0", "W11", "W12", "W13", "Xa0", "Xa1", "X11", "X10", "W15", "Xd0", "W16", "Xd1", "Xb1", "X21", "X20", "Xb0",
    "W17", "MB0", "W21", "MC0", "Xc1", "W22", "Xc0", "Xe1", "Y12", "X12", "X13", "Xe0", "W23", "Y13", "Xf1", "Y14",
    "X14", "Y15", "X15", "Xf0", "X16", "Y17", "X17", "Y16", "X22", "Y22", "X23", "W14", "Y23", "UP1", "Y24", "X24",
    "Y25", "X25", "UP0", "X26", "Y27", "X27", "X32", "Y32", "Y26", "X33", "Y33", "MD0", "X34", "Y34", "B10", "Y35",
    "B11", "X42", "Y42", "X43", "Y43", "X35", "Y36", "B20", "Y44", "X44", "Y45", "B21", "X36", "UP2", "Y37", "UP3",
    "X37", "Y46", "X45", "UP4", "W20", "B12", "X46", "Y47", "X47", "B13", "UP5", "B14", "B22", "DN0", "DN1", "UP6",
    "UP7", "B23", "B24", "B15", "DN2", "B16", "DN3", "B17", "DN4", "B25", "B26", "B27", "DN5", "DN6", "DN7",
]
EARLY = [0]


def softplus(v):
    e = jnp.exp(-jnp.abs(v))
    series = e * (1.0 - e * (1.0 / 2 - e * (1.0 / 3 - e * (1.0 / 4 - e * (1.0 / 5 - e / 6)))))
    return jnp.maximum(v, 0.0) + jnp.where(e < 0.03, series, jnp.log(1.0 + e))


def one_minus_exp(v):
    series = 1.0 + v / 8
    for n in (7, 6, 5, 4, 3, 2):
        series = 1.0 + v / n * series
    return jnp.where(v > -0.25, -v * series, 1.0 - jnp.exp(v))


def kernel(
    mix_in, moe_in, w_x, w_y, shift, w_gate, w_up, w_down,
    mix_gain, conv_taps, recur_w, input_w, logit, moe_gain, routes, weight,
    both_out,
    mix_v, moe_v, win_v, shift_v, gu_v, wd,
    mix_gain_v, conv_taps_v, recur_v, input_v, logit_v, moe_gain_v, routes_v, weight_v,
    c0, c1, sent, X, hown, H, res, ret, ybr, xb, xcv, halo_out, halo_in, sa, sb, carry_out, carry_in,
    load_sem, x_send, x_recv, b_send, b_recv, a_send, a_recv, w_send, w_recv, f_send, f_recv,
    d_send, d_recv, r_send, r_recv, k_send, k_recv, h_sem,
):
    ep, tp = lax.axis_index("ep"), lax.axis_index("tp")
    z, core = ep // CORES, lax.rem(ep, CORES)
    y, x = tp // SIDE, lax.rem(tp, SIDE)

    def wrap(v, n):
        return lax.rem(v + 2 * n, n)

    east, west = wrap(x + 1, SIDE), wrap(x - 1, SIDE)
    north, south = wrap(y + 1, SIDE), wrap(y - 1, SIDE)
    across = wrap(x + 2, SIDE)
    plane = [(ep, y * SIDE + east), (ep, y * SIDE + west), (ep, north * SIDE + x), (ep, south * SIDE + x)]
    row = [plane[0], plane[1], (ep, y * SIDE + across)]
    others = [(dx, wrap(y + dy, SIDE)) for dy in range(SIDE) for dx in range(SIDE) if dx or dy]

    def by_x(values, of):
        got = values[0]
        for n in range(1, SIDE):
            got = jnp.where(of == n, values[n], got)
        return got

    def offset(m, of):
        return by_x(NEAR[SIDE * m : SIDE * (m + 1)], of)

    def lanes(n):
        return pl.ds(pl.multiple_of(n * LANE, LANE), LANE)

    def peer(at, c):
        return wrap(z + NEAR[at], RING) * CORES + c

    loads = {}
    for n, (name, src, dst) in enumerate([
        ("routes", routes, routes_v), ("down", w_down.at[0], wd.at[:, lanes(x)]), ("moe_gain", moe_gain, moe_gain_v), ("moe", moe_in, moe_v),
        ("mix_gain", mix_gain, mix_gain_v), ("mix", mix_in, mix_v),
        ("w_x", w_x, win_v.at[:, :LANE]), ("w_y", w_y, win_v.at[:, LANE:]),
        ("taps", conv_taps, conv_taps_v), ("recur", recur_w, recur_v), ("input", input_w, input_v),
        ("logit", logit, logit_v), ("shift", shift, shift_v),
        ("gate", w_gate.at[0], gu_v.at[:, :LANE]), ("up", w_up.at[0], gu_v.at[:, LANE:]),
        ("weight", weight, weight_v),
    ]):
        loads[name] = pltpu.make_async_copy(src, dst, load_sem.at[n])
        loads[name].start()

    def loaded(*names):
        for name in names:
            loads[name].wait()

    barrier = pltpu.get_barrier_semaphore()

    def greet(where):
        pl.semaphore_signal(barrier, inc=1, device_id=where, device_id_type=MESH)

    far = sorted(range(1, RING), key=lambda at: -abs(NEAR[at]))
    for at in far:
        for c in range(CORES):
            greet((peer(at, c), tp))
    for m in sorted(range(RING // SIDE), key=lambda m: -max(map(abs, NEAR[SIDE * m : SIDE * (m + 1)]))):
        for by in range(1, SIDE):
            other = wrap(x + by, SIDE)
            for c in range(CORES):
                greet((wrap(z + offset(m, x), RING) * CORES + c, y * SIDE + other))
                greet((wrap(z - offset(m, other), RING) * CORES + c, y * SIDE + other))
    greet((peer(0, 1 - core), tp))
    for dx, its_y in others:
        greet((ep, its_y * SIDE + wrap(x + dx, SIDE)))
    greeted = len(others) + EP - 1 + 2 * RING // SIDE * (SIDE - 1) * CORES

    pending = []

    def launch(src, dst, ss, rs, where):
        copy = pltpu.make_async_remote_copy(
            src_ref=src, dst_ref=dst, send_sem=ss, recv_sem=rs, device_id=where, device_id_type=MESH
        )
        copy.start()
        pending.append(copy)
        return copy

    def normed(ref, gain, lanes):
        v = ref[...].astype(F32)
        scale = lax.rsqrt(jnp.sum(v * v, axis=1, keepdims=True) / D + epsilon)
        if lanes is not None:
            v = ref[:, lanes].astype(F32)
            return (v * scale * gain[:, lanes]).astype(BF16)
        return (v * scale * gain[...]).astype(BF16)

    def columns(ref):
        flat = ref[...].astype(F32)
        return jnp.transpose(jnp.concatenate([flat] * 4, axis=0))

    lane_e = lax.broadcasted_iota(jnp.int32, (ROWS, LANE), 1)
    loaded("routes")
    chosen = columns(routes_v).astype(jnp.int32)
    onehot = [jnp.where(chosen[:, k : k + 1] == lane_e, 1.0, 0.0).astype(BF16) for k in range(2)]
    before = jnp.where(
        lax.broadcasted_iota(jnp.int32, (ROWS, ROWS), 1) < lax.broadcasted_iota(jnp.int32, (ROWS, ROWS), 0), 1.0, 0.0
    ).astype(BF16)
    rank = [jnp.dot(before, hot, preferred_element_type=F32) for hot in onehot]
    rank[1] = rank[1] + jnp.sum(onehot[0].astype(F32), axis=0, keepdims=True)
    lane_1 = lax.broadcasted_iota(jnp.int32, (1, LANE), 1)
    off = (lane_1 // CORES - z + 2 * RING) % RING
    at = jnp.zeros((1, LANE), jnp.int32)
    for n in range(1, RING):
        at = jnp.where(off == NEAR[n] % RING, n, at)
    base = (CAP * place_of(at, lane_1 % CORES)).astype(F32)
    slot_lane = lax.broadcasted_iota(jnp.int32, (ROWS, SLOTS), 1)
    for ref, hot, r in zip((c0, c1), onehot, rank):
        slot = jnp.sum(hot.astype(F32) * (r + base), axis=1, keepdims=True).astype(jnp.int32)
        ref[...] = jnp.where(slot_lane == slot, 1.0, 0.0).astype(BF16)

    loaded("moe", "moe_gain")
    own_rows = normed(moe_v, moe_gain_v, lanes(tp))
    sent[...] = lax.dot_general(
        c0[...] + c1[...], own_rows, (((0,), (0,)), ((), ())), preferred_element_type=F32
    ).astype(BF16).reshape(EP, CAP, LANE)

    with jax.named_scope("barrier"):
        pl.semaphore_wait(barrier, greeted)
    loaded("down")
    ways, got = {}, set()

    def received(*key):
        if key not in got:
            got.add(key)
            ways[key].wait_recv()

    def weights(step, q):
        if step == 1:
            views = [(wd.at[pl.ds(q * WROWS, WROWS), lanes(x)], q)] * 2
        else:
            received("W", 1, q, 0)
            received("W", 1, q + PIECES // 2, 1)
            views = [
                (wd.at[pl.ds(q * WROWS, WROWS), lanes(west)], PIECES + q),
                (wd.at[pl.ds((q + PIECES // 2) * WROWS, WROWS), lanes(east)], PIECES + q),
            ]
        for n, (view, slot) in enumerate(views):
            ways["W", step, q, n] = launch(view, view, w_send.at[2 * slot + n], w_recv.at[2 * slot + n], row[n])

    for q in EARLY:
        weights(1, q)

    def block(buf, p):
        return buf.at[y, x, pl.ds(pl.multiple_of(p * CAP, CAP), CAP)]

    def dispatch(at, c):
        local = place_of(PLACE[-NEAR[at] % RING], c)
        place = place_of(at, core)
        where = wrap(z - NEAR[at], RING) * CORES + c
        launch(sent.at[local], block(X, place), d_send.at[local], d_recv.at[place], (where, tp))

    dispatch(0, 1 - core)
    for at in range(1, RING):
        for c in range(CORES):
            dispatch(at, c)
    mine = place_of(0, core)
    X[y, x, pl.ds(pl.multiple_of(mine * CAP, CAP), CAP), :] = sent[mine]

    def arrived(p, sem, ref):
        pltpu.make_async_remote_copy(
            src_ref=ref, dst_ref=ref, send_sem=sem.at[p], recv_sem=sem.at[p],
            device_id=(ep, tp), device_id_type=MESH,
        ).wait_recv()

    def await_dispatch(k):
        if ("in", k) in ways:
            return
        ways["in", k] = None
        for p in range(k * CH // CAP, (k + 1) * CH // CAP):
            if p % SIDE or k > 1:
                arrived(p, d_recv, block(X, p))
            else:

                @pl.when(mine != p)
                def _():
                    arrived(p, d_recv, block(X, p))

    def gather(part, step, k):
        lo, size = k * CH, XROWS[k]
        if part == "Y":
            lo, size = lo + size, CH - size
        if size == 0:
            return
        full, first, second = pl.ds(lo, size), pl.ds(lo, size // 2), pl.ds(lo + size // 2, size // 2)
        along_x = (part == "X") == (step < 3)
        if step == 1:
            await_dispatch(k)
            views = [X.at[y, x, full]] * 2
        elif step == 2 and along_x:
            views = [X.at[y, west, first], X.at[y, east, second]]
        elif step == 2:
            views = [X.at[south, x, first], X.at[north, x, second]]
        elif step == 3 and along_x:
            views = [X.at[:, x, full]] * 2
        elif step == 3:
            views = [X.at[y, :, full]] * 2
        elif along_x:
            views = [X.at[:, west, first], X.at[:, east, second]]
        else:
            views = [X.at[south, :, first], X.at[north, :, second]]
        if step == 3:
            for n in range(2):
                received(part, 2, k, n)
        for n in range(2):
            if step == 2 or step == 4:
                received(part, step - 1, k, n)
            slot = ((("XY".index(part) * CHUNKS) + k) * 4 + step - 1) * 2 + n
            ways[part, step, k, n] = launch(
                views[n], views[n], x_send.at[slot], x_recv.at[slot], plane[n if along_x else 2 + n]
            )

    def fine(letter, k):
        lo = k * CH
        full, first, second = pl.ds(lo, CH), pl.ds(lo, CH // 2), pl.ds(lo + CH // 2, CH // 2)
        stage, at = divmod("abcdef".index(letter), 3)
        cols = ([x], [west, east], [across])[at]
        if letter == "a":
            await_dispatch(k)
        for step in range(1, at + 1 if stage == 0 else 1):
            for n in range(2):
                received("X", step, k, n)
        for i, col in enumerate(cols):
            for n in range(2):
                if stage == 0:
                    view = X.at[y, col, full]
                else:
                    received("F", "abc"[at], k, i, n)
                    view = X.at[south, col, first] if n == 0 else X.at[north, col, second]
                slot = (FINE.index(k) * 6 + "abcdef".index(letter)) * 4 + 2 * i + n
                ways["F", letter, k, i, n] = launch(view, view, f_send.at[slot], f_recv.at[slot], plane[2 + n])

    def all_blocks(buf, rows):
        return jnp.concatenate([buf[a, b, rows, :] for a in range(SIDE) for b in range(SIDE)], axis=1)

    def quarter(k, n):
        return pl.ds(pl.multiple_of(k * CH + n * QROWS, QROWS), QROWS)

    def run_up(k):
        for part in "XY":
            for n in range(2):
                if (part, 4, k, n) in ways:
                    received(part, 4, k, n)
        for key in [key for key in ways if key[0] == "F" and key[1] in "def" and key[2] == k]:
            received(*key)
        if "up" not in ways:
            ways["up"] = loaded("gate", "up")
        both = jnp.dot(all_blocks(X, pl.ds(k * CH, CH)), gu_v[...], preferred_element_type=F32)
        g, u = both[:, :LANE], both[:, LANE:]
        hown[pl.ds(k * CH, CH), :] = (g * jax.nn.sigmoid(g) * u).astype(BF16)
        ours = pl.ds(k * QROWS, QROWS)
        if k in STRAIGHT:
            for n, (dx, its_y) in enumerate(others):
                slot = 3 * CHUNKS + STRAIGHT.index(k) * len(others) + n
                who = wrap(x + dx, SIDE)
                ways["S", k, n] = launch(
                    hown.at[quarter(k, who)], H.at[y, x, ours], a_send.at[slot], a_recv.at[slot], (ep, its_y * SIDE + who)
                )
        for n, who in enumerate(() if k in STRAIGHT else (east, west, across)):
            slot = 3 * k + n
            ways["A", k, n] = launch(hown.at[quarter(k, who)], H.at[y, x, ours], a_send.at[slot], a_recv.at[slot], row[n])
        H[y, x, ours, :] = hown[quarter(k, x), :]

    def spread(step, k):
        slot = 4 * k + 2 * (step - 1)
        lo = k * QROWS
        if step == 1:
            for n, who in enumerate((west, east, across)):
                received("A", k, n)
            views = [H.at[y, :, pl.ds(lo, QROWS)]] * 2
        else:
            views = [H.at[south, :, pl.ds(lo, QROWS // 2)], H.at[north, :, pl.ds(lo + QROWS // 2, QROWS // 2)]]
        for n in range(2):
            if step == 2:
                received("B", 1, k, n)
            ways["B", step, k, n] = launch(views[n], views[n], b_send.at[slot + n], b_recv.at[slot + n], plane[2 + n])

    def give(k, by, act):
        other, m = wrap(x + by, SIDE), k // 2
        place = by_x([place_of(PLACE[-v % RING], core) for v in NEAR[SIDE * m : SIDE * (m + 1)]], x)
        slot = k * SIDE + by
        copy = pltpu.make_async_remote_copy(
            src_ref=res.at[k, other], dst_ref=ret.at[place], send_sem=r_send.at[slot], recv_sem=r_recv.at[place],
            device_id=(wrap(z + offset(m, x), RING) * CORES + (x + k) % CORES, y * SIDE + other), device_id_type=MESH,
        )
        if k < CORES and by == 0:
            stays = jnp.logical_and(x == 0, core == k)

            @pl.when(jnp.logical_not(stays))
            def _():
                act(copy)

            if act is starts:

                @pl.when(stays)
                def _():
                    ret[mine] = res[k, 0]

        else:
            act(copy)

    def starts(copy):
        copy.start()

    def run_down(k):
        if k in STRAIGHT:
            for n in range(len(others)):
                received("S", k, n)
        for n in range(0 if k in STRAIGHT else 2):
            received("B", 2, k, n)
        if "down" not in ways:
            ways["down"] = None
            for q in range(PIECES // 2):
                received("W", 1, q, 1)
                received("W", 1, q + PIECES // 2, 0)
                received("W", 2, q, 0)
                received("W", 2, q, 1)
        out = jnp.dot(all_blocks(H, pl.ds(k * QROWS, QROWS)), wd[...], preferred_element_type=F32).astype(BF16)
        for n in range(SIDE):
            res[k, n] = out[:, n * LANE : (n + 1) * LANE]
        for by in range(SIDE):
            give(k, by, starts)

    def mix_a():
        loaded("mix", "mix_gain", "w_x", "w_y")
        rows = normed(mix_v, mix_gain_v, None)
        both = jnp.dot(rows, win_v[...], preferred_element_type=F32).astype(BF16)
        ybr[...] = both[:, LANE:]
        xb[pl.ds(8, ROWS), :] = both[:, :LANE].astype(F32)
        halo_out[...] = both[ROWS - 16 :, :LANE]
        ways["halo",] = launch(halo_out, halo_in, h_sem.at[0], h_sem.at[1], (wrap(ep + 1, EP), tp))

    def mix_b():
        received("halo")
        loaded("taps", "recur", "input", "logit", "shift")
        xb[pl.ds(0, 8), :] = jnp.where(ep > 0, halo_in[...].astype(F32)[8:], 0.0)
        conv = jnp.zeros((ROWS, LANE), F32)
        for k in range(4):
            conv = conv + conv_taps_v[k : k + 1, :] * xb[pl.ds(5 + k, ROWS), :]
        x_conv = conv.astype(BF16)
        xcv[...] = x_conv
        gate_a = jnp.dot(x_conv, recur_v[0], preferred_element_type=F32)
        gate_x = jnp.dot(x_conv, input_v[0], preferred_element_type=F32)
        log_decay = -lru_scale * jax.nn.sigmoid(gate_a) * softplus(-logit_v[...]) + shift_v[...]
        sa[...] = jnp.exp(log_decay)
        sb[...] = jnp.sqrt(one_minus_exp(2.0 * log_decay)) * jax.nn.sigmoid(gate_x) * x_conv.astype(F32)

    def mix_c():
        a, b = sa[...], sb[...]
        row = lax.broadcasted_iota(jnp.int32, (ROWS, LANE), 0)
        by = 1
        while by < ROWS:
            behind = row >= by
            b = jnp.where(behind, a * pltpu.roll(b, by, 0), 0.0) + b
            a = jnp.where(behind, pltpu.roll(a, by, 0), 1.0) * a
            by *= 2
        sa[...] = a
        sb[...] = b
        carry_out[0:1, :] = a[ROWS - 1 :, :]
        carry_out[1:2, :] = b[ROWS - 1 :, :]

        def tell(at, c):
            where = peer(at, c)
            launch(carry_out, carry_in.at[ep], k_send.at[CORES * at + c], k_recv.at[ep], (where, tp))

        tell(0, 1 - core)
        for at in range(1, RING):
            for c in range(CORES):
                tell(at, c)
        carry_in[ep] = carry_out[...]

    def mix_d():
        for at in range(RING):
            for c in range(CORES):
                if at > 0 or c == 0:
                    who = peer(at, c) if at else peer(0, 1 - core)
                    arrived(who, k_recv, carry_in.at[who])
        state = jnp.zeros((1, LANE), F32)
        for e in range(EP):
            pair = carry_in[e]
            state = jnp.where(e < ep, pair[0:1] * state + pair[1:2], state)
        lru = sb[...] + sa[...] * state
        both_out[0] = (lru * jax.nn.gelu(ybr[...].astype(F32), approximate=True)).astype(BF16)

    for item in ORDER:
        what, k = item[:2], int(item[2:])
        with jax.named_scope(f"{what}_{k}"):
            if what == "UP":
                run_up(k)
            elif what == "DN":
                run_down(k)
            elif what[0] == "M":
                {"A": mix_a, "B": mix_b, "C": mix_c, "D": mix_d}[what[1]]()
            elif what[0] == "W":
                weights(int(what[1]), k)
            elif what[0] == "B":
                spread(int(what[1]), k)
            elif what[1] in "abcdef":
                fine(what[1], k)
            else:
                gather(what[0], int(what[1]), k)

    with jax.named_scope("sends"):
        for copy in pending:
            copy.wait_send()
        for k in range(CHUNKS):
            for by in range(SIDE):
                give(k, by, lambda copy: copy.wait_send())
    loaded("weight")
    w = columns(weight_v)
    total = w[:, 0:1] + w[:, 1:2]
    picked = [jnp.zeros((ROWS, LANE), F32)] * 2
    for half in range(2):
        blocks = range(half * EP // 2, (half + 1) * EP // 2)
        with jax.named_scope(f"back_{half}"):
            for p in blocks:
                if p not in (0, SIDE):
                    arrived(p, r_recv, ret.at[p])
            if half == 0:
                arrived(SIDE - mine, r_recv, ret.at[SIDE - mine])

                @pl.when(x != 0)
                def _():
                    arrived(mine, r_recv, ret.at[mine])

        part = pl.ds(half * SLOTS // 2, SLOTS // 2)
        back = ret[pl.ds(half * EP // 2, EP // 2)].reshape(SLOTS // 2, LANE)
        for n, ref in enumerate((c0, c1)):
            picked[n] = picked[n] + jnp.dot(ref[:, part], back, preferred_element_type=F32)
    both_out[1] = (w[:, 0:1] / total * picked[0] + w[:, 1:2] / total * picked[1]).astype(BF16)


def local(
    mix_in, mix_gain, w_in_x, w_in_y, conv_taps, recur_gate_w, input_gate_w, decay_logit, decay_shift,
    moe_in, moe_gain, routes, route_weight, expert_gate, expert_up, expert_down,
):
    hbm = pl.BlockSpec(memory_space=pltpu.HBM)
    vmem = pl.BlockSpec(memory_space=pltpu.VMEM)
    dma = pltpu.SemaphoreType.DMA
    out = jax.ShapeDtypeStruct((2, ROWS, LANE), BF16)
    v = pltpu.VMEM
    fines = 24 * len(FINE)
    straight = CHUNKS * 3 + len(STRAIGHT) * (SIDE * SIDE - 1)
    both = pl.pallas_call(
        kernel,
        out_shape=out,
        in_specs=[hbm] * 16,
        out_specs=vmem,
        scratch_shapes=[
            v((ROWS, D), BF16), v((ROWS, D), BF16), v((D, 2 * LANE), BF16), v((ROWS, LANE), F32),
            v((D, 2 * LANE), BF16), v((D, SIDE * LANE), BF16),
            v((1, D), F32), v((4, LANE), F32), v((1, LANE, LANE), BF16), v((1, LANE, LANE), BF16), v((1, LANE), F32),
            v((1, D), F32), v((2, ROWS), jnp.int32), v((2, ROWS), F32),
            v((ROWS, SLOTS), BF16), v((ROWS, SLOTS), BF16), v((EP, CAP, LANE), BF16),
            v((SIDE, SIDE, SLOTS, LANE), BF16), v((SLOTS, LANE), BF16), v((SIDE, SIDE, SLOTS // SIDE, LANE), BF16),
            v((CHUNKS, SIDE, CAP, LANE), BF16), v((EP, CAP, LANE), BF16),
            v((ROWS, LANE), BF16), v((ROWS + 8, LANE), F32), v((ROWS, LANE), BF16),
            v((16, LANE), BF16), v((16, LANE), BF16), v((ROWS, LANE), F32), v((ROWS, LANE), F32),
            v((2, LANE), F32), v((EP, 2, LANE), F32),
            dma((16,)), dma((CHUNKS * 16,)), dma((CHUNKS * 16,)), dma((CHUNKS * 4,)), dma((CHUNKS * 4,)),
            dma((straight,)), dma((straight,)), dma((PIECES * 3,)), dma((PIECES * 3,)), dma((fines,)), dma((fines,)), dma((EP,)), dma((EP,)),
            dma((EP,)), dma((EP,)), dma((EP,)), dma((EP,)), dma((2,)),
        ],
        compiler_params=pltpu.CompilerParams(
            collective_id=0, has_side_effects=True, vmem_limit_bytes=67043328
        ),
        name="mixer_and_experts",
    )(
        mix_in, moe_in, w_in_x, w_in_y, decay_shift, expert_gate, expert_up, expert_down,
        mix_gain.reshape(1, D), conv_taps, recur_gate_w, input_gate_w, decay_logit.reshape(1, LANE),
        moe_gain.reshape(1, D), routes.T, route_weight.T,
    )
    return both[0], both[1]


def solution(mesh):
    placed = (
        P("ep", None),
        P(),
        P(None, "tp"),
        P(None, "tp"),
        P(None, "tp"),
        P("tp", None, None),
        P("tp", None, None),
        P("tp"),
        P("ep", "tp"),
        P("ep", None),
        P(),
        P("ep", None),
        P("ep", None),
        P("ep", None, "tp"),
        P("ep", None, "tp"),
        P("ep", None, "tp"),
    )
    return jax.shard_map(
        local, mesh=mesh, in_specs=placed, out_specs=(P("ep", "tp"), P("ep", "tp")), check_vma=False
    )
```
